512 devices in a mesh: sp: 64 (over z, y), fs: 4 (over x), tp: 2 (over core).
Axes of the slice: x: 4, y: 8, z: 8, core: 2. Of those that a mesh axis runs over, the one named last changes fastest.
Arguments:
- tokens: bfloat16 [4, 8192, 2048], P('fs', ('sp', 'tp')), may hold values from -6 to 6
- input_norm_gain: float32 [2048], replicated, may hold values from 0.1 to 1.9
- pooling_input_weight: bfloat16 [2048, 1024], P('sp', 'tp'), may hold values from -0.125 to 0.125
- query_weight: bfloat16 [2048, 1024], P('sp', 'tp'), may hold values from -0.125 to 0.125
- forget_weight: bfloat16 [2048, 1024], P('sp', 'tp'), may hold values from -0.125 to 0.125
- value_weight: bfloat16 [2048, 1024], P('sp', 'tp'), may hold values from -0.125 to 0.125
- pooling_group_maps: bfloat16 [4, 256, 256], P('tp'), may hold values from -0.375 to 0.375
- pooling_scale: float32 [1024], P('tp'), may hold values from 0.1 to 1.9
- lower_bound_logits: float32 [1024], P('tp')
- decay_spike: float32 [4, 8192, 8], P('fs', 'sp', 'tp'), may hold values from -0.75 to 0
- head_norm_gain: float32 [1024], P('tp'), may hold values from 0.1 to 1.9
- pooling_output_weight: bfloat16 [1024, 2048], P('tp', 'sp'), may hold values from -0.125 to 0.125
- recurrent_output_weight: bfloat16 [1024, 2048], P('tp', 'sp'), may hold values from -0.125 to 0.125
Outputs:
- mixed: bfloat16 [4, 8192, 2048], P('fs', ('sp', 'tp'))
The draws below stay inside these ranges and needn't reach their ends.
All inputs are finite; a program needn't handle non-finite values.
Results may differ from the reference program's by a relative error of at most 0.013.
Values may be sent and summed in bfloat16 or wider, within the bound.
A program may use at most 64 MiB of HBM per device.

```python
import jax
import jax.numpy as jnp
from jax import lax

D = 2048
POOL_GROUP = 256
POOL_GROUPS = 4
HEAD = 128
RECURRENT_HEADS = 8
BLOCK = 64
TOK_DEV = 128
D_POOL = 1024
D_REC = 1024
LEN = 8192
SEQUENCE_COUNT = 4
N_TP = 2


def head_kinds(key):
    ranking = jax.random.permutation(jax.random.fold_in(key, 11), RECURRENT_HEADS)
    return ranking < RECURRENT_HEADS // 2


def draw_lower_bound_logits(key, part):
    lasting = head_kinds(key)
    spread = jax.random.uniform(jax.random.fold_in(key, 12), (RECURRENT_HEADS, HEAD), jnp.float32)
    slow_rate = 0.3 * jnp.exp(jnp.log(4.0) * spread) / LEN
    fast_rate = 0.03 * jnp.exp(jnp.log(10.0 / 3.0) * spread)
    chosen = jnp.where(lasting[:, None], slow_rate, fast_rate)
    return (jnp.log1p(-chosen) - jnp.log(chosen)).reshape(D_REC)


def draw_decay_spike(key, part):
    lasting = head_kinds(key)
    devices = LEN // TOK_DEV
    spread = jax.random.uniform(jax.random.fold_in(key, 21), (SEQUENCE_COUNT, devices, RECURRENT_HEADS), jnp.float32)
    fast_rate = 0.004 * jnp.exp(jnp.log(5.0) * spread)
    slow_rate = 0.1 * jnp.exp(jnp.log(6.0) * spread) / LEN
    local_decay_rate = jnp.repeat(jnp.where(lasting[None, None, :], slow_rate, fast_rate), TOK_DEV, axis=1)
    third_length = LEN // 3
    spike_locations = jax.random.randint(jax.random.fold_in(key, 22), (SEQUENCE_COUNT, 3, RECURRENT_HEADS), 0, third_length)
    spike_locations = spike_locations + third_length * jnp.arange(3, dtype=jnp.int32)[None, :, None]
    kept_fraction = jax.random.uniform(jax.random.fold_in(key, 23), (SEQUENCE_COUNT, 3, RECURRENT_HEADS), jnp.float32, 0.55, 0.8)
    position_index = jnp.arange(LEN, dtype=jnp.int32)
    agreement = (position_index[None, :, None, None] == spike_locations[:, None, :, :]).astype(jnp.float32)
    spikes = jnp.sum(agreement * jnp.log(kept_fraction)[:, None, :, :], axis=2)
    return spikes - local_decay_rate


def shard_levels(own_key, shape, split, smallest, largest):
    level, own = 1.0, jax.random.fold_in(own_key, 6)
    for axis_at, blocks in split:
        steps = jnp.exp(jax.random.uniform(jax.random.fold_in(own, axis_at), (blocks,), jnp.float32, smallest / len(split), largest / len(split)))
        level = level * jnp.repeat(steps, shape[axis_at] // blocks).reshape([-1 if axis == axis_at else 1 for axis in range(len(shape))])
    return level


def scatter_about(rng, dims, scale, bound, shards=(), kind=jnp.bfloat16):
    drawn = jax.random.normal(rng, dims, jnp.float32) * scale
    if len(shards) > 0:
        drawn = shard_levels(rng, dims, shards, -0.22, 0.18) * drawn
    return jnp.clip(drawn, min=-bound, max=bound).astype(kind)


def setup_inputs(seed: int = 0) -> dict:
    seeds = jax.random.split(jax.random.key(seed), 14)
    return {
        "tokens": scatter_about(seeds[0], (SEQUENCE_COUNT, LEN, D), 1.0, 6.0, ((0, 4), (1, 128))),
        "input_norm_gain": jnp.clip(1.0 + 0.18 * jax.random.normal(seeds[1], (D,), jnp.float32), 0.1, 1.9),
        "pooling_input_weight": scatter_about(seeds[2], (D, D_POOL), D ** -0.5, 0.125, ((0, 64), (1, 2))),
        "query_weight": scatter_about(seeds[3], (D, D_REC), D ** -0.5, 0.125, ((0, 64), (1, 2))),
        "forget_weight": scatter_about(seeds[4], (D, D_REC), D ** -0.5, 0.125, ((0, 64), (1, 2))),
        "value_weight": scatter_about(seeds[5], (D, D_REC), D ** -0.5, 0.125, ((0, 64), (1, 2))),
        "pooling_group_maps": scatter_about(seeds[6], (POOL_GROUPS, POOL_GROUP, POOL_GROUP), POOL_GROUP ** -0.5, 0.375, ((0, 2),)),
        "pooling_scale": jnp.clip(1.0 + 0.18 * jax.random.normal(seeds[7], (D_POOL,), jnp.float32), 0.1, 1.9),
        "lower_bound_logits": draw_lower_bound_logits(jax.random.fold_in(seeds[13], 71), 0),
        "decay_spike": draw_decay_spike(jax.random.fold_in(seeds[13], 71), 0),
        "head_norm_gain": jnp.clip(1.0 + 0.18 * jax.random.normal(seeds[10], (D_REC,), jnp.float32), 0.1, 1.9),
        "pooling_output_weight": scatter_about(seeds[11], (D_POOL, D), (D_POOL + D_REC) ** -0.5, 0.125, ((0, 2), (1, 64))),
        "recurrent_output_weight": scatter_about(seeds[12], (D_REC, D), (D_POOL + D_REC) ** -0.5, 0.125, ((0, 2), (1, 64))),
    }


EPSILON = 1e-06
HIGHEST = lax.Precision.HIGHEST

def stored(values):
    return lax.optimization_barrier(values.astype(jnp.bfloat16))

def rms_scale(values, gain):
    return values * lax.rsqrt(lax.optimization_barrier(jnp.mean(values * values, axis=-1, keepdims=True)) + EPSILON) * gain

def pooling(pool_input, pooling_group_maps, pooling_scale):
    length_total = pool_input.shape[0]
    groups = pooling_group_maps.shape[0]
    group_size = pooling_group_maps.shape[1]
    reach_rows = 2 ** groups
    padded = jnp.pad(pool_input.astype(jnp.float32).reshape(length_total, groups, group_size), ((reach_rows, 0), (0, 0), (0, 0)))
    windows = 2 ** (jnp.arange(groups, dtype=jnp.int32) + 1)
    window_sum = jnp.zeros((length_total, groups, group_size), jnp.float32)
    for offset in range(reach_rows):
        inside = (offset < windows).astype(jnp.float32)
        window_sum = window_sum + padded[reach_rows - offset:reach_rows - offset + length_total] * inside[:, None]
    counts = jnp.minimum(jnp.arange(length_total, dtype=jnp.int32)[:, None] + 1, windows[None, :]).astype(jnp.float32)
    pool_diff = stored(window_sum / counts[:, :, None] - padded[reach_rows:])
    mapped = jnp.einsum('tgc,gcd->tgd', pool_diff.astype(jnp.float32), pooling_group_maps.astype(jnp.float32))
    return (mapped.reshape(length_total, groups * group_size) * pooling_scale).astype(jnp.bfloat16)

def linear_recurrence(query_matrix, forget_gate_logit, value_projected, lower_bound_logits, spike_row, head_norm_gain):
    length_total, width = query_matrix.shape
    number_heads = spike_row.shape[1]
    head_width = width // number_heads
    block_layout = (length_total // BLOCK, BLOCK, number_heads, head_width)
    reader = jax.nn.silu(query_matrix.astype(jnp.float32)).reshape(block_layout)
    key_gate_value = jax.nn.sigmoid(-lower_bound_logits) * jax.nn.sigmoid(-forget_gate_logit.astype(jnp.float32))
    decay_logarithm = (jnp.log1p(-key_gate_value).reshape(length_total, number_heads, head_width) + spike_row[:, :, None]).reshape(block_layout)
    key_rows = key_gate_value.reshape(block_layout)
    value_rows = value_projected.astype(jnp.float32).reshape(block_layout)
    causal = (jnp.arange(BLOCK)[:, None] >= jnp.arange(BLOCK)[None, :]).astype(jnp.float32)

    def advance(carried, input_batch):
        block_reader, block_key, block_value, block_log = input_batch
        inner_log = jnp.cumsum(block_log, axis=0)
        read_scaled = block_reader * jnp.exp(inner_log)
        key_scaled = block_key * jnp.exp(-inner_log)
        scores = jnp.einsum('thd,shd->hts', read_scaled, key_scaled, precision=HIGHEST) * causal
        output = jnp.einsum('hts,she->the', scores, block_value, precision=HIGHEST)
        output = output + jnp.einsum('thd,hde->the', read_scaled, carried, precision=HIGHEST)
        closing = inner_log[-1]
        key_tail = block_key * jnp.exp(closing[None] - inner_log)
        carried = jnp.exp(closing)[:, :, None] * carried + jnp.einsum('shd,she->hde', key_tail, block_value, precision=HIGHEST)
        return (carried, output)
    initial = jnp.zeros((number_heads, head_width, head_width), jnp.float32)
    final_state, read_out = lax.scan(advance, initial, (reader, key_rows, value_rows, decay_logarithm))
    read_out = read_out.reshape(length_total, number_heads, head_width)
    return (rms_scale(read_out, 1.0).reshape(length_total, width) * head_norm_gain).astype(jnp.bfloat16)

def reference(tokens, input_norm_gain, pooling_input_weight, query_weight, forget_weight, value_weight, pooling_group_maps, pooling_scale, lower_bound_logits, decay_spike, head_norm_gain, pooling_output_weight, recurrent_output_weight):
    pool_width = pooling_input_weight.shape[1] // N_TP
    rec_width = query_weight.shape[1] // N_TP

    def sequence_tokens(input_batch):
        token_series, spike_row = input_batch
        normed = rms_scale(token_series.astype(jnp.float32), input_norm_gain).astype(jnp.bfloat16)
        pool_input = stored(jnp.dot(normed, pooling_input_weight, preferred_element_type=jnp.float32))
        query_matrix = stored(jnp.dot(normed, query_weight, preferred_element_type=jnp.float32))
        forget_gate_logit = stored(jnp.dot(normed, forget_weight, preferred_element_type=jnp.float32))
        value_projected = stored(jnp.dot(normed, value_weight, preferred_element_type=jnp.float32))
        pool_out = pooling(pool_input, pooling_group_maps, pooling_scale)
        recurrent_output = linear_recurrence(query_matrix, forget_gate_logit, value_projected, lower_bound_logits, spike_row, head_norm_gain)
        mixed_sum = jnp.zeros((token_series.shape[0], pooling_output_weight.shape[1]), jnp.float32)
        for member in range(N_TP):
            pool_lo = member * pool_width
            rec_lo = member * rec_width
            partial_value = jnp.dot(pool_out[:, pool_lo:pool_lo + pool_width], pooling_output_weight[pool_lo:pool_lo + pool_width], preferred_element_type=jnp.float32)
            partial_value = partial_value + jnp.dot(recurrent_output[:, rec_lo:rec_lo + rec_width], recurrent_output_weight[rec_lo:rec_lo + rec_width], preferred_element_type=jnp.float32)
            mixed_sum = mixed_sum + stored(partial_value).astype(jnp.float32)
        return mixed_sum.astype(jnp.bfloat16)
    return lax.map(sequence_tokens, (tokens, decay_spike))
```

```python
import functools

import jax
import jax.numpy as jnp
from jax import lax
from jax.experimental import pallas as pl
from jax.experimental.pallas import tpu as pltpu
from jax.sharding import Mesh
from jax.sharding import PartitionSpec as P

MESH = pl.DeviceIdType.MESH
BLOCK = 64
HEAD = 128
TOK = 128
HALF = 64
WROWS = 16
WCOLS = 256
HALO = 16
EPS = 1e-06
F32 = jnp.float32
BF16 = jnp.bfloat16


def three_parts(value):
    high = value.astype(BF16)
    rest = value - high.astype(F32)
    mid = rest.astype(BF16)
    low = (rest - mid.astype(F32)).astype(BF16)
    return high, mid, low


def nt(a, b):
    return lax.dot_general(a, b, (((1,), (1,)), ((), ())), preferred_element_type=F32)


def tn(a, b):
    return lax.dot_general(a, b, (((0,), (0,)), ((), ())), preferred_element_type=F32)


def nn(a, b):
    return jnp.dot(a, b, preferred_element_type=F32)


def kernel(
    sizes,
    tok_ref,
    gin_ref,
    wp_ref,
    wq_ref,
    wf_ref,
    wv_ref,
    maps_ref,
    scale_ref,
    lb_ref,
    spike_ref,
    hg_ref,
    wpo_ref,
    wro_ref,
    out_ref,
    tokbuf,
    wbuf,
    wobuf,
    wop,
    wor,
    spbuf,
    fbuf,
    vbuf,
    qbuf,
    pbuf,
    cfull,
    inner_buf,
    c1_send,
    c1_recv,
    pex,
    dex,
    c2_send,
    c2_recv,
    c3_send,
    c3_recv,
    halo,
    within,
    xpool,
    xrec,
    pacc,
    parts,
    part_in,
    mixed,
    obuf,
    p1_ss,
    p1_rs,
    p2_ss,
    p2_rs,
    tok_ss,
    tok_rs,
    d2d_ss,
    d2d_rs,
    sp_ss,
    sp_rs,
    c1_ss,
    c1_rs,
    c2_ss,
    c2_rs,
    c3_ss,
    c3_rs,
    halo_ss,
    halo_rs,
    xp_ss,
    xp_rs,
    xr_ss,
    xr_rs,
    part_ss,
    part_rs,
    o_ss,
    o_rs,
):
    nz, ny, nx = sizes
    z, y, x, c = (lax.axis_index(name) for name in ("z", "y", "x", "c"))
    sp = z * ny + y
    width = tok_ref.shape[2]
    wo_cols = 32 // nx
    piece = HEAD // ny
    packed = nx * piece
    half_pool = nx * HEAD

    def rc(src, dst, ss, rs, **device):
        return pltpu.make_async_remote_copy(
            src_ref=src, dst_ref=dst, send_sem=ss, recv_sem=rs, device_id=device, device_id_type=MESH
        )

    def at(base, step, count):
        return lax.rem(base + step + count, count)

    barrier = pltpu.get_barrier_semaphore()

    def greet(**device):
        pl.semaphore_signal(barrier, inc=1, device_id=device, device_id_type=MESH)

    for k in range(1, ny):
        greet(y=at(y, k, ny))
    for k in range(1, nz):
        greet(z=at(z, k, nz))
    for k in range(1, nx):
        greet(x=at(x, k, nx))
    greet(c=1 - c)
    if nz > 1 and ny > 1:
        down = jnp.logical_and(y == ny - 1, z < nz - 1)
        up = jnp.logical_and(y == 0, z > 0)

        @pl.when(down)
        def _():
            greet(z=z + 1, y=0)

        @pl.when(up)
        def _():
            greet(z=z - 1, y=ny - 1)

    own = tok_ref[0].astype(F32)
    square = jnp.mean(own * own, axis=-1, keepdims=True)
    tokbuf[x, c] = (own * lax.rsqrt(square + EPS) * gin_ref[...]).astype(BF16)
    lanes = pl.ds(pl.multiple_of(x * HEAD, HEAD), HEAD)
    for p in range(2):
        rows = slice(p * WROWS, (p + 1) * WROWS)
        wbuf[0, z, y, p, :, 0:HEAD] = wf_ref[rows, lanes]
        wbuf[0, z, y, p, :, HEAD:WCOLS] = wv_ref[rows, lanes]
        wbuf[1, z, y, p, :, 0:HEAD] = wp_ref[rows, lanes]
        wbuf[1, z, y, p, :, HEAD:WCOLS] = wq_ref[rows, lanes]
    heads = spike_ref.shape[2]
    pick = (
        lax.broadcasted_iota(jnp.int32, (8, heads), 0)
        == lax.broadcasted_iota(jnp.int32, (8, heads), 1)
    ).astype(F32)
    spbuf[x] = lax.dot_general(
        pick,
        spike_ref[0],
        (((1,), (1,)), ((), ())),
        precision=lax.Precision.HIGHEST,
        preferred_element_type=F32,
    )

    greeted = (ny - 1) + (nz - 1) + (nx - 1) + 1
    if nz > 1 and ny > 1:
        at_end = (y // (ny - 1)) * (1 - z // (nz - 1))
        at_start = ((ny - 1 - y) // (ny - 1)) * (1 - (nz - 1 - z) // (nz - 1))
        greeted = greeted + at_end + at_start
    pl.semaphore_wait(barrier, greeted)

    def p1(st, k, path):
        if path == 0:
            return lambda zz, zt: rc(
                wbuf.at[st, zz, y, 0],
                wbuf.at[st, zz, y, 0],
                p1_ss.at[st, 0, k - 1],
                p1_rs.at[st, 0, k - 1],
                z=zt,
            )
        return lambda yy, yt: rc(
            wbuf.at[st, z, yy, 1],
            wbuf.at[st, z, yy, 1],
            p1_ss.at[st, 1, k - 1],
            p1_rs.at[st, 1, k - 1],
            y=yt,
        )

    def p1_send(st):
        for k in range(1, max(nz, ny)):
            if k < nz:
                p1(st, k, 0)(z, at(z, k, nz)).start()
            if k < ny:
                p1(st, k, 1)(y, at(y, k, ny)).start()

    def p1_wait(st):
        for k in range(1, nz):
            p1(st, k, 0)(at(z, -k, nz), at(z, -k, nz)).wait_recv()
        for k in range(1, ny):
            p1(st, k, 1)(at(y, -k, ny), at(y, -k, ny)).wait_recv()

    def p1_done(st):
        for k in range(1, nz):
            p1(st, k, 0)(z, at(z, k, nz)).wait_send()
        for k in range(1, ny):
            p1(st, k, 1)(y, at(y, k, ny)).wait_send()

    routes = []
    for path, count in ((0, ny), (1, nz)):
        for way in range(2):
            routes.append((path, way, count // 2 if way == 0 else (count - 1) // 2))

    def p2(st, path, way, step, distance, to):
        sign = 1 if way == 0 else -1
        if path == 0:
            block = wbuf.at[st, :, at(y, -sign * distance, ny), 0]
            device = {"y": at(y, sign * to, ny)}
        else:
            block = wbuf.at[st, at(z, -sign * distance, nz), :, 1]
            device = {"z": at(z, sign * to, nz)}
        return rc(
            block, block, p2_ss.at[st, path, way, step], p2_rs.at[st, path, way, step], **device
        )

    steps = max(r[2] for r in routes)

    def p2_send(st, step):
        for path, way, count in routes:
            if step < count:
                p2(st, path, way, step, step, 1).start()

    def p2_wait(st, step):
        for path, way, count in routes:
            if step < count:
                p2(st, path, way, step, step + 1, 1).wait_recv()

    def p2_advance(st, step):
        for path, way, count in routes:
            if step - 1 < count:
                p2(st, path, way, step - 1, step, 1).wait_recv()
            if step < count:
                p2(st, path, way, step, step, 1).start()

    def p2_done(st):
        for path, way, count in routes:
            for step in range(count):
                p2(st, path, way, step, step, 1).wait_send()

    right, left, across = at(x, 1, nx), at(x, -1, nx), at(x, 2, nx)

    def ring_x(part, ss, rs):
        def move(slot, owner, half, to):
            return rc(part(owner, half), part(owner, half), ss.at[slot], rs.at[slot], x=to)

        class Ring:
            def start_first(self):
                move(0, x, 0, right).start()
                move(2, x, 1, left).start()

            def start_second(self):
                move(1, x, 1, right).start()
                move(3, x, 0, left).start()

            def start(self):
                self.start_first()
                self.start_second()

            def forward(self):
                move(0, left, 0, right).wait_recv()
                move(4, left, 0, right).start()
                move(2, right, 1, left).wait_recv()
                move(5, right, 1, left).start()

            def near(self):
                move(1, left, 1, right).wait_recv()
                move(3, right, 0, left).wait_recv()

            def far(self):
                move(4, across, 0, right).wait_recv()
                move(5, across, 1, left).wait_recv()

            def done(self):
                for slot, owner, half, to in (
                    (0, x, 0, right),
                    (1, x, 1, right),
                    (2, x, 1, left),
                    (3, x, 0, left),
                    (4, left, 0, right),
                    (5, right, 1, left),
                ):
                    move(slot, owner, half, to).wait_send()

        return Ring()

    tokens = ring_x(
        lambda owner, half: tokbuf.at[owner, c, pl.ds(half * (HALF // 2), HALF // 2)], tok_ss, tok_rs
    )

    def to_partner(slot, owner, core):
        return rc(
            tokbuf.at[owner, core], tokbuf.at[owner, core], d2d_ss.at[slot], d2d_rs.at[slot], c=1 - c
        )

    def spikes(k, owner):
        return rc(spbuf.at[owner], spbuf.at[owner], sp_ss.at[k - 1], sp_rs.at[k - 1], x=at(x, k, nx))

    p1_send(0)
    tokens.start()
    to_partner(0, x, c).start()
    for k in range(1, nx):
        spikes(k, x).start()
    p1_send(1)

    wobuf[0] = wpo_ref[...].astype(F32).T
    wobuf[1] = wro_ref[...].astype(F32).T
    mine = pl.ds(pl.multiple_of(x * wo_cols, wo_cols), wo_cols)
    block = jnp.concatenate([wobuf[0, mine, :], wobuf[1, mine, :]], axis=0).astype(BF16)
    for p in range(2):
        wbuf[2, z, y, p] = block[:, p * WCOLS : (p + 1) * WCOLS]

    p1_wait(0)
    p2_send(0, 0)
    tokens.forward()
    p1_wait(1)
    p2_send(1, 0)
    tokens.near()
    to_partner(1, left, c).start()
    to_partner(2, right, c).start()
    p1_send(2)
    for step in range(1, steps):
        p2_advance(0, step)
        p2_advance(1, step)
        if step == 1:
            tokens.far()
            to_partner(3, across, c).start()
    for slot, owner in enumerate((x, left, right, across)):
        to_partner(slot, owner, 1 - c).wait_recv()
    for k in range(1, nx):
        spikes(k, at(x, -k, nx)).wait_recv()
    p2_wait(0, steps - 1)

    rows = nx * TOK

    def project(st):
        return nn(tokbuf[...].reshape(rows, width), wbuf[st].reshape(width, WCOLS)).astype(BF16)

    projected = project(0)
    fbuf[...] = projected[:, :HEAD]
    vbuf[...] = projected[:, HEAD:]

    ti = lax.broadcasted_iota(jnp.int32, (TOK, TOK), 0)
    si = lax.broadcasted_iota(jnp.int32, (TOK, TOK), 1)
    same = (ti // BLOCK) == (si // BLOCK)
    causal = jnp.logical_and(same, ti >= si)
    lower = causal.astype(F32)
    lower_b = lower.astype(BF16)
    ones_b = jnp.ones((TOK, HEAD), BF16)
    second = lax.broadcasted_iota(jnp.int32, (TOK, HEAD), 0) >= BLOCK
    lb_gate = 1.0 / (1.0 + jnp.exp(lb_ref[pl.ds(x, 1), :]))
    decays = []
    for s in range(nx):
        span = slice(s * TOK, (s + 1) * TOK)
        key = lb_gate * (1.0 / (1.0 + jnp.exp(fbuf[span, :].astype(F32))))
        logs = three_parts(jnp.log1p(-key))
        spike_row = spbuf[s, pl.ds(x, 1), :]
        spread = three_parts(lower * spike_row)
        inner = nn(
            jnp.concatenate([lower_b, lower_b, lower_b, *spread], axis=1),
            jnp.concatenate([*logs, ones_b, ones_b, ones_b], axis=0),
        )
        first_end = inner[BLOCK - 1 : BLOCK, :]
        total = first_end + inner[TOK - 1 : TOK, :]
        full = inner + jnp.where(second, first_end, 0.0)
        inner_buf[span, :] = inner
        cfull[span, :] = full
        tail = (key * jnp.exp(total - full)).astype(BF16)
        state = tn(vbuf[span, :], tail).astype(BF16)
        for j in range(ny):
            c1_send[j, s * piece : (s + 1) * piece, :] = state[j * piece : (j + 1) * piece, :]
        decays.append(jnp.exp(total))

    def decay_rows(values):
        out = []
        for value in values:
            high = value.astype(BF16).astype(F32)
            out += [high, value - high]
        out.append(jnp.zeros((16 - len(out), HEAD), F32))
        return jnp.concatenate(out, axis=0).astype(BF16)

    extra = decay_rows(decays)
    for j in range(ny):
        c1_send[j, packed : packed + 16, :] = extra
    c1_recv[y] = c1_send[y]

    def c1(k, slot):
        to = at(y, k, ny)
        return rc(c1_send.at[to], c1_recv.at[slot], c1_ss.at[k - 1], c1_rs.at[k - 1], y=to)

    for k in range(1, ny):
        c1(k, y).start()

    p1_wait(2)
    p2_wait(1, steps - 1)
    p2_send(2, 0)
    projected = project(1)
    pbuf[...] = projected[:, :HEAD].reshape(nx, TOK, HEAD)
    qbuf[...] = projected[:, HEAD:]

    last = nz * ny - 1
    halo_src = pbuf.at[:, TOK - HALO : TOK]

    def halo_copy(**device):
        return rc(halo_src, halo, halo_ss, halo_rs, **device)

    if ny > 1:

        @pl.when(y < ny - 1)
        def _():
            halo_copy(y=y + 1).start()

    if nz > 1:

        @pl.when(jnp.logical_and(y == ny - 1, z < nz - 1))
        def _():
            halo_copy(z=z + 1, y=0).start()

    @pl.when(sp == 0)
    def _():
        halo[...] = jnp.zeros_like(halo)

    for k in range(1, ny):
        c1(k, at(y, -k, ny)).wait_recv()

    def read_decay(block, s):
        at_row = packed + 2 * s
        return block[at_row : at_row + 1, :] + block[at_row + 1 : at_row + 2, :]

    run = [jnp.zeros((piece, HEAD), F32) for _ in range(nx)]
    fade = [jnp.ones((1, HEAD), F32) for _ in range(nx)]
    for j in range(ny):
        block = c1_recv[j].astype(F32)
        for s in range(nx):
            pex[j, s * piece : (s + 1) * piece, :] = run[s]
            dex[j, s : s + 1, :] = fade[s]
            decay = read_decay(block, s)
            run[s] = decay * run[s] + block[s * piece : (s + 1) * piece, :]
            fade[s] = fade[s] * decay
    c2_send[0:packed, :] = jnp.concatenate(run, axis=0).astype(BF16)
    c2_send[packed : packed + 16, :] = decay_rows(fade)

    def c2(k, slot, to):
        return rc(c2_send, c2_recv.at[slot], c2_ss.at[k - 1], c2_rs.at[k - 1], z=to)

    if nz > 1:

        def send_later(k, _):
            c2(k, z, z + k).start()
            return _

        lax.fori_loop(1, nz - z, send_later, 0)

    for s in range(nx):
        span = slice(s * TOK, (s + 1) * TOK)
        query = qbuf[span, :].astype(F32)
        reader = query * (1.0 / (1.0 + jnp.exp(-query)))
        key = lb_gate * (1.0 / (1.0 + jnp.exp(fbuf[span, :].astype(F32))))
        inner = inner_buf[span, :]
        scaled = (reader * jnp.exp(inner)).astype(BF16)
        near = (key * jnp.exp(-inner)).astype(BF16)
        tail = (
            key[:BLOCK] * jnp.exp(inner[BLOCK - 1 : BLOCK, :] - inner[:BLOCK])
        ).astype(BF16)
        scores = nt(scaled, jnp.concatenate([near, tail], axis=0))
        cross = jnp.concatenate([scores[:, TOK:], scores[:, TOK:]], axis=1)
        before = jnp.logical_and(ti >= BLOCK, si < BLOCK)
        chosen = jnp.where(causal, scores[:, :TOK], jnp.where(before, cross, 0.0))
        within[span, :] = nn(chosen.astype(BF16), vbuf[span, :])
        cfull[span, :] = reader * jnp.exp(cfull[span, :])
    if steps > 1:
        p2_advance(2, 1)

    if ny > 1:

        @pl.when(y > 0)
        def _():
            halo_copy(y=y - 1).wait_recv()

    if nz > 1:

        @pl.when(jnp.logical_and(y == 0, z > 0))
        def _():
            halo_copy(z=z - 1, y=ny - 1).wait_recv()

    group = (c * half_pool + x * HEAD) // WCOLS
    window = jnp.where(group == 0, 2, jnp.where(group == 1, 4, jnp.where(group == 2, 8, 16)))
    band = jnp.logical_and(ti >= si, ti - si < window).astype(BF16)
    hi = lax.broadcasted_iota(jnp.int32, (TOK, HALO), 0)
    hj = lax.broadcasted_iota(jnp.int32, (TOK, HALO), 1)
    band_before = (hi + HALO - hj < window).astype(BF16)
    place = sp * TOK + lax.broadcasted_iota(jnp.int32, (TOK, HEAD), 0) + 1
    count = jnp.minimum(place, window).astype(F32)
    for s in range(nx):
        sums = nn(band, pbuf[s]) + nn(band_before, halo[s])
        xpool[x, s * TOK : (s + 1) * TOK, :] = (sums / count - pbuf[s].astype(F32)).astype(BF16)

    half_rows = rows // 2
    pool_ring = ring_x(
        lambda owner, half: xpool.at[owner, pl.ds(half * half_rows, half_rows)], xp_ss, xp_rs
    )
    rec_ring = ring_x(
        lambda owner, half: xrec.at[owner, pl.ds(half * half_rows, half_rows)], xr_ss, xr_rs
    )
    pool_ring.start()

    def add_row(zz, carry):
        if nz > 1:
            rc(
                c2_send, c2_recv.at[zz], c2_ss.at[z - zz - 1], c2_rs.at[z - zz - 1], z=zz
            ).wait_recv()
        block = c2_recv[zz].astype(F32)
        out = []
        for s in range(nx):
            out.append(
                read_decay(block, s) * carry[s] + block[s * piece : (s + 1) * piece, :]
            )
        return tuple(out)

    earlier = tuple(jnp.zeros((piece, HEAD), F32) for _ in range(nx))
    if nz > 1:
        earlier = lax.fori_loop(0, z, add_row, earlier)
    for j in range(ny):
        for s in range(nx):
            span = slice(s * piece, (s + 1) * piece)
            c3_send[j, span, :] = (dex[j, s : s + 1, :] * earlier[s] + pex[j, span, :]).astype(BF16)
    c3_recv[y] = c3_send[y]

    def c3(k, slot):
        to = at(y, k, ny)
        return rc(c3_send.at[to], c3_recv.at[slot], c3_ss.at[k - 1], c3_rs.at[k - 1], y=to)

    for k in range(1, ny):
        c3(k, y).start()

    pool_ring.forward()
    for step in range(2, steps):
        p2_advance(2, step)
    p2_wait(2, steps - 1)
    for p in range(2):
        both = wbuf[2, :, :, p].reshape(nz * ny, 2 * wo_cols, WCOLS).astype(F32)
        cols = slice(p * WCOLS, (p + 1) * WCOLS)
        wop[:, cols] = both[:, :wo_cols].reshape(nz * ny * wo_cols, WCOLS).astype(BF16)
        wor[:, cols] = both[:, wo_cols:].reshape(nz * ny * wo_cols, WCOLS).astype(BF16)

    for k in range(1, ny):
        c3(k, at(y, -k, ny)).wait_recv()
    gain = hg_ref[pl.ds(x, 1), :]

    def finish(s):
        span = slice(s * TOK, (s + 1) * TOK)
        prior = c3_recv[:, s * piece : (s + 1) * piece, :].reshape(HEAD, HEAD)
        read = within[span, :] + nt(cfull[span, :].astype(BF16), prior)
        square = jnp.mean(read * read, axis=-1, keepdims=True)
        xrec[x, span, :] = (read * lax.rsqrt(square + EPS) * gain).astype(BF16)

    for s in range(nx):
        finish(s)
    rec_ring.start()

    pool_ring.near()
    pool_ring.far()
    pieces = []
    for g in range(half_pool // WCOLS):
        cols = slice(g * WCOLS, (g + 1) * WCOLS)
        diff = jnp.concatenate([xpool[2 * g], xpool[2 * g + 1]], axis=1)
        pieces.append((nn(diff, maps_ref[g]) * scale_ref[:, cols]).astype(BF16))
    rec_ring.forward()
    pacc[...] = nt(jnp.concatenate(pieces, axis=1), wop[...])
    rec_ring.near()
    rec_ring.far()
    rec = jnp.concatenate([xrec[i] for i in range(nx)], axis=1)
    cols_out = nz * ny * wo_cols
    parts[...] = (
        (pacc[...] + nt(rec, wor[...])).astype(BF16).reshape(nx, 2, HALF, cols_out)
    )

    def to_half(s):
        return rc(parts.at[s, 1 - c], part_in.at[s], part_ss.at[s], part_rs.at[s], c=1 - c)

    for s in range(nx):
        to_half(s).start()

    def deliver(k, owner):
        to = at(x, k, nx)
        return rc(mixed.at[to], obuf.at[owner], o_ss.at[k - 1], o_rs.at[k - 1], x=to)

    for s in range(nx):
        to_half(s).wait_recv()
        mixed[s] = (parts[s, c].astype(F32) + part_in[s].astype(F32)).astype(BF16)
    for k in range(1, nx):
        deliver(k, x).start()
    obuf[x] = mixed[x]
    for k in range(1, nx):
        deliver(k, at(x, -k, nx)).wait_recv()

    chunk = min(HEAD, cols_out)
    total_cols = chunk * nx
    src = lax.broadcasted_iota(jnp.int32, (total_cols, total_cols), 0)
    dst = lax.broadcasted_iota(jnp.int32, (total_cols, total_cols), 1)
    wanted = (
        lax.div(lax.rem(dst, 32), wo_cols) * chunk
        + lax.div(dst, 32) * wo_cols
        + lax.rem(dst, wo_cols)
    )
    order = (src == wanted).astype(BF16)
    for q in range(cols_out // chunk):
        cols = slice(q * chunk, (q + 1) * chunk)
        joined = jnp.concatenate([obuf[i, :, cols] for i in range(nx)], axis=1)
        out_ref[0, :, q * total_cols : (q + 1) * total_cols] = nn(joined, order).astype(BF16)

    for st in range(3):
        p1_done(st)
        p2_done(st)
    tokens.done()
    pool_ring.done()
    rec_ring.done()
    for slot, owner in enumerate((x, left, right, across)):
        to_partner(slot, owner, c).wait_send()
    for k in range(1, nx):
        spikes(k, x).wait_send()
        deliver(k, x).wait_send()
    for k in range(1, ny):
        c1(k, y).wait_send()
        c3(k, y).wait_send()
    if nz > 1:

        def sent_later(k, _):
            c2(k, z, z + k).wait_send()
            return _

        lax.fori_loop(1, nz - z, sent_later, 0)
    for s in range(nx):
        to_half(s).wait_send()

    @pl.when(sp < last)
    def _():
        halo_copy(c=1 - c).wait_send()


def body(sizes, *arrays):
    nz, ny, nx = sizes
    (tok, gin, wp, wq, wf, wv, maps, scale, lb, spike, hg, wpo, wro) = arrays
    width = tok.shape[2]
    rows = nx * TOK
    piece = HEAD // ny
    packed = nx * piece
    wo_cols = 32 // nx
    cols_out = nz * ny * wo_cols
    kdim = nx * HEAD
    steps = max(ny // 2, nz // 2)
    ring = [pltpu.SemaphoreType.DMA((6,))] * 2
    scratch = [
        pltpu.VMEM((nx, 2, HALF, width), BF16),
        pltpu.VMEM((3, nz, ny, 2, WROWS, WCOLS), BF16),
        pltpu.VMEM((2, 32, kdim), F32),
        pltpu.VMEM((cols_out, kdim), BF16),
        pltpu.VMEM((cols_out, kdim), BF16),
        pltpu.VMEM((nx, 8, TOK), F32),
        pltpu.VMEM((rows, HEAD), BF16),
        pltpu.VMEM((rows, HEAD), BF16),
        pltpu.VMEM((rows, HEAD), BF16),
        pltpu.VMEM((nx, TOK, HEAD), BF16),
        pltpu.VMEM((rows, HEAD), F32),
        pltpu.VMEM((rows, HEAD), F32),
        pltpu.VMEM((ny, packed + 16, HEAD), BF16),
        pltpu.VMEM((ny, packed + 16, HEAD), BF16),
        pltpu.VMEM((ny, packed, HEAD), F32),
        pltpu.VMEM((ny, 8, HEAD), F32),
        pltpu.VMEM((packed + 16, HEAD), BF16),
        pltpu.VMEM((nz, packed + 16, HEAD), BF16),
        pltpu.VMEM((ny, packed, HEAD), BF16),
        pltpu.VMEM((ny, packed, HEAD), BF16),
        pltpu.VMEM((nx, HALO, HEAD), BF16),
        pltpu.VMEM((rows, HEAD), F32),
        pltpu.VMEM((nx, rows, HEAD), BF16),
        pltpu.VMEM((nx, rows, HEAD), BF16),
        pltpu.VMEM((rows, cols_out), F32),
        pltpu.VMEM((nx, 2, HALF, cols_out), BF16),
        pltpu.VMEM((nx, HALF, cols_out), BF16),
        pltpu.VMEM((nx, HALF, cols_out), BF16),
        pltpu.VMEM((nx, HALF, cols_out), BF16),
        *[pltpu.SemaphoreType.DMA((3, 2, max(nz, ny) - 1))] * 2,
        *[pltpu.SemaphoreType.DMA((3, 2, 2, steps))] * 2,
        *ring,
        *[pltpu.SemaphoreType.DMA((nx,))] * 2,
        *[pltpu.SemaphoreType.DMA((nx - 1,))] * 2,
        *[pltpu.SemaphoreType.DMA((max(ny - 1, 1),))] * 2,
        *[pltpu.SemaphoreType.DMA((max(nz - 1, 1),))] * 2,
        *[pltpu.SemaphoreType.DMA((max(ny - 1, 1),))] * 2,
        *[pltpu.SemaphoreType.DMA] * 2,
        *ring,
        *ring,
        *[pltpu.SemaphoreType.DMA((nx,))] * 2,
        *[pltpu.SemaphoreType.DMA((nx - 1,))] * 2,
    ]
    return pl.pallas_call(
        functools.partial(kernel, sizes),
        out_shape=jax.ShapeDtypeStruct(tok.shape, BF16),
        in_specs=[pl.BlockSpec(memory_space=pltpu.VMEM)] * 13,
        out_specs=pl.BlockSpec(memory_space=pltpu.VMEM),
        scratch_shapes=scratch,
        compiler_params=pltpu.CompilerParams(
            collective_id=0, has_side_effects=True, vmem_limit_bytes=56 * 1024 * 1024
        ),
        name="layer",
    )(
        tok,
        gin.reshape(1, width),
        wp,
        wq,
        wf,
        wv,
        maps,
        scale.reshape(1, kdim),
        lb.reshape(nx, HEAD),
        spike,
        hg.reshape(nx, HEAD),
        wpo,
        wro,
    )


def layout(devices, sizes):
    nz, ny, nx = sizes
    torus = Mesh(devices.reshape(nz, ny, nx, 2), ("z", "y", "x", "c"))
    sp = ("z", "y")
    return jax.shard_map(
        functools.partial(body, sizes),
        mesh=torus,
        in_specs=(
            P("x", ("z", "y", "c"), None),
            P(),
            P(sp, "c"),
            P(sp, "c"),
            P(sp, "c"),
            P(sp, "c"),
            P("c", None, None),
            P("c"),
            P("c"),
            P("x", sp, "c"),
            P("c"),
            P("c", sp),
            P("c", sp),
        ),
        out_specs=P("x", ("z", "y", "c"), None),
        check_vma=False,
    )


def solution(mesh):
    return layout(mesh.devices, (8, 8, mesh.shape["fs"]))
```

```python
import functools

import jax
import jax.numpy as jnp
from jax import lax
from jax.experimental import pallas as pl
from jax.experimental.pallas import tpu as pltpu
from jax.sharding import Mesh
from jax.sharding import PartitionSpec as P

MESH = pl.DeviceIdType.MESH
BLOCK = 64
HEAD = 128
TOK = 128
HALF = 64
WROWS = 16
WCOLS = 256
HALO = 16
PARTS = 2
EPS = 1e-06
F32 = jnp.float32
BF16 = jnp.bfloat16


def three_parts(value):
    high = value.astype(BF16)
    rest = value - high.astype(F32)
    mid = rest.astype(BF16)
    low = (rest - mid.astype(F32)).astype(BF16)
    return high, mid, low


def nt(a, b):
    return lax.dot_general(a, b, (((1,), (1,)), ((), ())), preferred_element_type=F32)


def tn(a, b):
    return lax.dot_general(a, b, (((0,), (0,)), ((), ())), preferred_element_type=F32)


def nn(a, b):
    return jnp.dot(a, b, preferred_element_type=F32)


def kernel(
    sizes,
    tok_hbm,
    gin_hbm,
    wp_hbm,
    wq_hbm,
    wf_hbm,
    wv_hbm,
    maps_hbm,
    scale_hbm,
    lb_hbm,
    spike_hbm,
    hg_hbm,
    wpo_hbm,
    wro_hbm,
    out_ref,
    tok_ref,
    gin_ref,
    maps_ref,
    scale_ref,
    lb_ref,
    spike_ref,
    hg_ref,
    wo_ref,
    tokbuf,
    wbuf,
    wobuf,
    wop,
    wor,
    spbuf,
    fbuf,
    vbuf,
    qbuf,
    pbuf,
    cfull,
    inner_buf,
    c1_send,
    c1_recv,
    pex,
    dex,
    c2_send,
    c2_recv,
    c3_send,
    c3_recv,
    halo,
    within,
    xpool,
    xrec,
    pacc,
    parts,
    part_in,
    mixed,
    obuf,
    p1_ss,
    p1_rs,
    p2_ss,
    p2_rs,
    tok_ss,
    tok_rs,
    d2d_ss,
    d2d_rs,
    sp_ss,
    sp_rs,
    c1_ss,
    c1_rs,
    c2_ss,
    c2_rs,
    c3_ss,
    c3_rs,
    halo_ss,
    halo_rs,
    xp_ss,
    xp_rs,
    xr_ss,
    xr_rs,
    part_ss,
    part_rs,
    o_ss,
    o_rs,
    in_sems,
):
    nz, ny, nx = sizes
    z, y, x, c = (lax.axis_index(name) for name in ("z", "y", "x", "c"))
    sp = z * ny + y
    width = tok_hbm.shape[2]
    wo_cols = 32 // nx
    piece = HEAD // ny
    packed = nx * piece
    half_pool = nx * HEAD

    def rc(src, dst, ss, rs, **device):
        return pltpu.make_async_remote_copy(
            src_ref=src, dst_ref=dst, send_sem=ss, recv_sem=rs, device_id=device, device_id_type=MESH
        )

    def far_first(count):
        return sorted(range(1, count), key=lambda k: -min(k, count - k))

    def at(base, step, count):
        return lax.rem(base + step + count, count)

    pltpu.make_async_copy(tok_hbm, tok_ref, in_sems.at[0]).start()
    lanes = pl.ds(pl.multiple_of(x * HEAD, HEAD), HEAD)
    slices = []
    for n, ref in enumerate((wf_hbm, wv_hbm, wp_hbm, wq_hbm)):
        for p in range(2):
            slices.append(
                pltpu.make_async_copy(
                    ref.at[p * WROWS : (p + 1) * WROWS, lanes],
                    wbuf.at[n // 2, z, y, p, :, pl.ds((n % 2) * HEAD, HEAD)],
                    in_sems.at[1 + 2 * n + p],
                )
            )
    small = [
        pltpu.make_async_copy(src, dst, in_sems.at[9 + n])
        for n, (src, dst) in enumerate(
            (
                (gin_hbm, gin_ref),
                (spike_hbm, spike_ref),
                (wpo_hbm, wo_ref.at[0]),
                (wro_hbm, wo_ref.at[1]),
                (lb_hbm, lb_ref),
                (hg_hbm, hg_ref),
                (scale_hbm, scale_ref),
                (maps_hbm, maps_ref),
            )
        )
    ]
    for copy in slices[:4] + small[:2] + slices[4:] + small[2:]:
        copy.start()

    barrier = pltpu.get_barrier_semaphore()

    def greet(**device):
        pl.semaphore_signal(barrier, inc=1, device_id=device, device_id_type=MESH)

    for k in range(1, ny):
        greet(y=at(y, k, ny))
    for k in range(1, nz):
        greet(z=at(z, k, nz))
    for k in range(1, nx):
        greet(x=at(x, k, nx))
    greet(c=1 - c)
    if nz > 1 and ny > 1:
        down = jnp.logical_and(y == ny - 1, z < nz - 1)
        up = jnp.logical_and(y == 0, z > 0)

        @pl.when(down)
        def _():
            greet(z=z + 1, y=0)

        @pl.when(up)
        def _():
            greet(z=z - 1, y=ny - 1)

    pltpu.make_async_copy(tok_hbm, tok_ref, in_sems.at[0]).wait()
    small[0].wait()
    own = tok_ref[0].astype(F32)
    square = jnp.mean(own * own, axis=-1, keepdims=True)
    tokbuf[x, c] = (own * lax.rsqrt(square + EPS) * gin_ref[...]).astype(BF16)
    small[1].wait()
    spbuf[x] = spike_ref[0]
    for copy in slices:
        copy.wait()

    greeted = (ny - 1) + (nz - 1) + (nx - 1) + 1
    if nz > 1 and ny > 1:
        at_end = (y // (ny - 1)) * (1 - z // (nz - 1))
        at_start = ((ny - 1 - y) // (ny - 1)) * (1 - (nz - 1 - z) // (nz - 1))
        greeted = greeted + at_end + at_start
    pl.semaphore_wait(barrier, greeted)

    def p1(st, k, path):
        if path == 0:
            return lambda zz, zt: rc(
                wbuf.at[st, zz, y, 0],
                wbuf.at[st, zz, y, 0],
                p1_ss.at[st, 0, k - 1],
                p1_rs.at[st, 0, k - 1],
                z=zt,
            )
        return lambda yy, yt: rc(
            wbuf.at[st, z, yy, 1],
            wbuf.at[st, z, yy, 1],
            p1_ss.at[st, 1, k - 1],
            p1_rs.at[st, 1, k - 1],
            y=yt,
        )

    def p1_send(st):
        for k in far_first(max(nz, ny)):
            if k < nz:
                p1(st, k, 0)(z, at(z, k, nz)).start()
            if k < ny:
                p1(st, k, 1)(y, at(y, k, ny)).start()

    def p1_wait(st):
        for k in range(1, nz):
            p1(st, k, 0)(at(z, -k, nz), at(z, -k, nz)).wait_recv()
        for k in range(1, ny):
            p1(st, k, 1)(at(y, -k, ny), at(y, -k, ny)).wait_recv()

    def p1_done(st):
        for k in range(1, nz):
            p1(st, k, 0)(z, at(z, k, nz)).wait_send()
        for k in range(1, ny):
            p1(st, k, 1)(y, at(y, k, ny)).wait_send()

    paths = ((0, ny, nz), (1, nz, ny))

    def p2(st, path, way, source, distance, part):
        sign = 1 if way == 0 else -1
        if path == 0:
            size = nz // PARTS
            block = wbuf.at[st, pl.ds(part * size, size), at(y, -sign * source, ny), 0]
            device = {"y": at(y, sign * max(distance - source, 1), ny)}
        else:
            size = ny // PARTS
            block = wbuf.at[st, at(z, -sign * source, nz), pl.ds(part * size, size), 1]
            device = {"z": at(z, sign * max(distance - source, 1), nz)}
        where = (st, path, way, distance - 1, part)
        return rc(block, block, p2_ss.at[where], p2_rs.at[where], **device)

    def far_way(part):
        return 0 if part < PARTS // 2 else 1

    def each(part):
        return [(path, way, part) for path in range(2) for way in range(2)]

    def p2_own(st):
        for part in range(PARTS):
            for distance in (2, 1):
                for path, way, _ in each(part):
                    p2(st, path, way, 0, distance, part).start()

    def p2_relay(st):
        for part in range(PARTS):
            for path, way, _ in each(part):
                p2(st, path, way, 2, 2, part).wait_recv()
                if way == far_way(part):
                    p2(st, path, way, 2, 4, part).start()
                p2(st, path, way, 2, 3, part).start()

    def p2_wait(st):
        for part in range(PARTS):
            for path, way, _ in each(part):
                p2(st, path, way, 1, 1, part).wait_recv()
                p2(st, path, way, 3, 3, part).wait_recv()
                if way == far_way(part):
                    p2(st, path, way, 4, 4, part).wait_recv()

    def p2_done(st):
        for part in range(PARTS):
            for path, way, _ in each(part):
                for distance in (1, 2, 3, 4):
                    if distance < 4 or way == far_way(part):
                        p2(st, path, way, 0, distance, part).wait_send()

    right, left, across = at(x, 1, nx), at(x, -1, nx), at(x, 2, nx)

    def ring_x(part, ss, rs):
        def move(slot, owner, half, to):
            return rc(part(owner, half), part(owner, half), ss.at[slot], rs.at[slot], x=to)

        class Ring:
            def start_first(self):
                move(0, x, 0, right).start()
                move(2, x, 1, left).start()

            def start_second(self):
                move(1, x, 1, right).start()
                move(3, x, 0, left).start()

            def start(self):
                self.start_first()
                self.start_second()

            def forward(self):
                move(0, left, 0, right).wait_recv()
                move(4, left, 0, right).start()
                move(2, right, 1, left).wait_recv()
                move(5, right, 1, left).start()

            def near(self):
                move(1, left, 1, right).wait_recv()
                move(3, right, 0, left).wait_recv()

            def far(self):
                move(4, across, 0, right).wait_recv()
                move(5, across, 1, left).wait_recv()

            def done(self):
                for slot, owner, half, to in (
                    (0, x, 0, right),
                    (1, x, 1, right),
                    (2, x, 1, left),
                    (3, x, 0, left),
                    (4, left, 0, right),
                    (5, right, 1, left),
                ):
                    move(slot, owner, half, to).wait_send()

        return Ring()

    tokens = ring_x(
        lambda owner, half: tokbuf.at[owner, c, pl.ds(half * (HALF // 2), HALF // 2)], tok_ss, tok_rs
    )

    def to_partner(slot, owner, core):
        return rc(
            tokbuf.at[owner, core], tokbuf.at[owner, core], d2d_ss.at[slot], d2d_rs.at[slot], c=1 - c
        )

    def spikes(k, owner):
        return rc(spbuf.at[owner], spbuf.at[owner], sp_ss.at[k - 1], sp_rs.at[k - 1], x=at(x, k, nx))

    p1_send(0)
    tokens.start()
    to_partner(0, x, c).start()
    for k in range(1, nx):
        spikes(k, x).start()
    p1_send(1)

    for copy in small[2:]:
        copy.wait()
    wobuf[...] = wo_ref[...].astype(F32)
    mine = pl.ds(pl.multiple_of(x * wo_cols, wo_cols), wo_cols)
    block = jnp.concatenate([wobuf[0, mine, :], wobuf[1, mine, :]], axis=0).astype(BF16)
    for p in range(2):
        wbuf[2, z, y, p] = block[:, p * WCOLS : (p + 1) * WCOLS]

    p1_wait(0)
    p2_own(0)
    tokens.forward()
    tokens.near()
    to_partner(1, left, c).start()
    to_partner(2, right, c).start()
    p2_relay(0)
    p1_wait(1)
    p2_own(1)
    p1_send(2)
    tokens.far()
    to_partner(3, across, c).start()
    for slot, owner in enumerate((x, left, right, across)):
        to_partner(slot, owner, 1 - c).wait_recv()
    for k in range(1, nx):
        spikes(k, at(x, -k, nx)).wait_recv()
    p2_wait(0)

    rows = nx * TOK

    def project(st):
        return nn(tokbuf[...].reshape(rows, width), wbuf[st].reshape(width, WCOLS)).astype(BF16)

    projected = project(0)
    fbuf[...] = projected[:, :HEAD]
    vbuf[...] = projected[:, HEAD:]

    ti = lax.broadcasted_iota(jnp.int32, (TOK, TOK), 0)
    si = lax.broadcasted_iota(jnp.int32, (TOK, TOK), 1)
    same = (ti // BLOCK) == (si // BLOCK)
    causal = jnp.logical_and(same, ti >= si)
    lower = causal.astype(F32)
    lower_b = lower.astype(BF16)
    ones_b = jnp.ones((TOK, HEAD), BF16)
    second = lax.broadcasted_iota(jnp.int32, (TOK, HEAD), 0) >= BLOCK
    lb_gate = 1.0 / (1.0 + jnp.exp(lb_ref[pl.ds(x, 1), :]))
    decays = []
    for s in range(nx):
        span = slice(s * TOK, (s + 1) * TOK)
        key = lb_gate * (1.0 / (1.0 + jnp.exp(fbuf[span, :].astype(F32))))
        logs = three_parts(jnp.log1p(-key))
        spike_row = spbuf[s, pl.ds(x, 1), :]
        spread = three_parts(lower * spike_row)
        inner = nn(
            jnp.concatenate([lower_b, lower_b, lower_b, *spread], axis=1),
            jnp.concatenate([*logs, ones_b, ones_b, ones_b], axis=0),
        )
        first_end = inner[BLOCK - 1 : BLOCK, :]
        total = first_end + inner[TOK - 1 : TOK, :]
        full = inner + jnp.where(second, first_end, 0.0)
        inner_buf[span, :] = inner
        cfull[span, :] = full
        tail = (key * jnp.exp(total - full)).astype(BF16)
        state = tn(vbuf[span, :], tail).astype(BF16)
        for j in range(ny):
            c1_send[j, s * piece : (s + 1) * piece, :] = state[j * piece : (j + 1) * piece, :]
        decays.append(jnp.exp(total))

    def decay_rows(values):
        out = []
        for value in values:
            high = value.astype(BF16).astype(F32)
            out += [high, value - high]
        out.append(jnp.zeros((16 - len(out), HEAD), F32))
        return jnp.concatenate(out, axis=0).astype(BF16)

    extra = decay_rows(decays)
    for j in range(ny):
        c1_send[j, packed : packed + 16, :] = extra
    c1_recv[y] = c1_send[y]

    def c1(k, slot):
        to = at(y, k, ny)
        return rc(c1_send.at[to], c1_recv.at[slot], c1_ss.at[k - 1], c1_rs.at[k - 1], y=to)

    for k in far_first(ny):
        c1(k, y).start()

    p2_relay(1)

    for k in range(1, ny):
        c1(k, at(y, -k, ny)).wait_recv()

    def read_decay(block, s):
        at_row = packed + 2 * s
        return block[at_row : at_row + 1, :] + block[at_row + 1 : at_row + 2, :]

    run = [jnp.zeros((piece, HEAD), F32) for _ in range(nx)]
    fade = [jnp.ones((1, HEAD), F32) for _ in range(nx)]
    for j in range(ny):
        block = c1_recv[j].astype(F32)
        for s in range(nx):
            pex[j, s * piece : (s + 1) * piece, :] = run[s]
            dex[j, s : s + 1, :] = fade[s]
            decay = read_decay(block, s)
            run[s] = decay * run[s] + block[s * piece : (s + 1) * piece, :]
            fade[s] = fade[s] * decay
    c2_send[0:packed, :] = jnp.concatenate(run, axis=0).astype(BF16)
    c2_send[packed : packed + 16, :] = decay_rows(fade)

    def c2(k, slot, to):
        return rc(c2_send, c2_recv.at[slot], c2_ss.at[k - 1], c2_rs.at[k - 1], z=to)

    if nz > 1:

        def send_later(k, _):
            c2(k, z, z + k).start()
            return _

        lax.fori_loop(1, nz - z, send_later, 0)

    p1_wait(2)
    p2_own(2)
    p2_wait(1)
    projected = project(1)
    pbuf[...] = projected[:, :HEAD].reshape(nx, TOK, HEAD)
    qbuf[...] = projected[:, HEAD:]

    last = nz * ny - 1
    halo_src = pbuf.at[:, TOK - HALO : TOK]

    def halo_copy(**device):
        return rc(halo_src, halo, halo_ss, halo_rs, **device)

    if ny > 1:

        @pl.when(y < ny - 1)
        def _():
            halo_copy(y=y + 1).start()

    if nz > 1:

        @pl.when(jnp.logical_and(y == ny - 1, z < nz - 1))
        def _():
            halo_copy(z=z + 1, y=0).start()

    @pl.when(sp == 0)
    def _():
        halo[...] = jnp.zeros_like(halo)

    for s in range(nx):
        span = slice(s * TOK, (s + 1) * TOK)
        query = qbuf[span, :].astype(F32)
        reader = query * (1.0 / (1.0 + jnp.exp(-query)))
        key = lb_gate * (1.0 / (1.0 + jnp.exp(fbuf[span, :].astype(F32))))
        inner = inner_buf[span, :]
        scaled = (reader * jnp.exp(inner)).astype(BF16)
        near = (key * jnp.exp(-inner)).astype(BF16)
        tail = (
            key[:BLOCK] * jnp.exp(inner[BLOCK - 1 : BLOCK, :] - inner[:BLOCK])
        ).astype(BF16)
        scores = nt(scaled, jnp.concatenate([near, tail], axis=0))
        cross = jnp.concatenate([scores[:, TOK:], scores[:, TOK:]], axis=1)
        before = jnp.logical_and(ti >= BLOCK, si < BLOCK)
        chosen = jnp.where(causal, scores[:, :TOK], jnp.where(before, cross, 0.0))
        within[span, :] = nn(chosen.astype(BF16), vbuf[span, :])
        cfull[span, :] = reader * jnp.exp(cfull[span, :])
    if ny > 1:

        @pl.when(y > 0)
        def _():
            halo_copy(y=y - 1).wait_recv()

    if nz > 1:

        @pl.when(jnp.logical_and(y == 0, z > 0))
        def _():
            halo_copy(z=z - 1, y=ny - 1).wait_recv()

    group = (c * half_pool + x * HEAD) // WCOLS
    window = jnp.where(group == 0, 2, jnp.where(group == 1, 4, jnp.where(group == 2, 8, 16)))
    band = jnp.logical_and(ti >= si, ti - si < window).astype(BF16)
    hi = lax.broadcasted_iota(jnp.int32, (TOK, HALO), 0)
    hj = lax.broadcasted_iota(jnp.int32, (TOK, HALO), 1)
    band_before = (hi + HALO - hj < window).astype(BF16)
    place = sp * TOK + lax.broadcasted_iota(jnp.int32, (TOK, HEAD), 0) + 1
    count = jnp.minimum(place, window).astype(F32)
    for s in range(nx):
        sums = nn(band, pbuf[s]) + nn(band_before, halo[s])
        xpool[x, s * TOK : (s + 1) * TOK, :] = (sums / count - pbuf[s].astype(F32)).astype(BF16)

    half_rows = rows // 2
    pool_ring = ring_x(
        lambda owner, half: xpool.at[owner, pl.ds(half * half_rows, half_rows)], xp_ss, xp_rs
    )
    rec_ring = ring_x(
        lambda owner, half: xrec.at[owner, pl.ds(half * half_rows, half_rows)], xr_ss, xr_rs
    )
    pool_ring.start()

    def add_row(zz, carry):
        if nz > 1:
            rc(
                c2_send, c2_recv.at[zz], c2_ss.at[z - zz - 1], c2_rs.at[z - zz - 1], z=zz
            ).wait_recv()
        block = c2_recv[zz].astype(F32)
        out = []
        for s in range(nx):
            out.append(
                read_decay(block, s) * carry[s] + block[s * piece : (s + 1) * piece, :]
            )
        return tuple(out)

    earlier = tuple(jnp.zeros((piece, HEAD), F32) for _ in range(nx))
    if nz > 1:
        earlier = lax.fori_loop(0, z, add_row, earlier)
    for j in range(ny):
        for s in range(nx):
            span = slice(s * piece, (s + 1) * piece)
            c3_send[j, span, :] = (dex[j, s : s + 1, :] * earlier[s] + pex[j, span, :]).astype(BF16)
    c3_recv[y] = c3_send[y]

    def c3(k, slot):
        to = at(y, k, ny)
        return rc(c3_send.at[to], c3_recv.at[slot], c3_ss.at[k - 1], c3_rs.at[k - 1], y=to)

    for k in far_first(ny):
        c3(k, y).start()

    pool_ring.forward()
    p2_relay(2)
    for k in range(1, ny):
        c3(k, at(y, -k, ny)).wait_recv()
    gain = hg_ref[pl.ds(x, 1), :]

    def finish(s):
        span = slice(s * TOK, (s + 1) * TOK)
        prior = c3_recv[:, s * piece : (s + 1) * piece, :].reshape(HEAD, HEAD)
        read = within[span, :] + nt(cfull[span, :].astype(BF16), prior)
        square = jnp.mean(read * read, axis=-1, keepdims=True)
        xrec[x, span, :] = (read * lax.rsqrt(square + EPS) * gain).astype(BF16)

    for s in range(nx):
        finish(s)
    rec_ring.start()
    pool_ring.near()
    pool_ring.far()
    pieces = []
    for g in range(half_pool // WCOLS):
        cols = slice(g * WCOLS, (g + 1) * WCOLS)
        diff = jnp.concatenate([xpool[2 * g], xpool[2 * g + 1]], axis=1)
        pieces.append((nn(diff, maps_ref[g]) * scale_ref[:, cols]).astype(BF16))
    rec_ring.forward()
    p2_wait(2)
    for p in range(2):
        both = wbuf[2, :, :, p].reshape(nz * ny, 2 * wo_cols, WCOLS).astype(F32)
        cols = slice(p * WCOLS, (p + 1) * WCOLS)
        wop[:, cols] = both[:, :wo_cols].reshape(nz * ny * wo_cols, WCOLS).astype(BF16)
        wor[:, cols] = both[:, wo_cols:].reshape(nz * ny * wo_cols, WCOLS).astype(BF16)
    pacc[...] = nt(jnp.concatenate(pieces, axis=1), wop[...])
    rec_ring.near()
    rec_ring.far()
    cols_out = nz * ny * wo_cols

    def to_half(s):
        return rc(parts.at[s, 1 - c], part_in.at[s], part_ss.at[s], part_rs.at[s], c=1 - c)

    def deliver(k, owner):
        to = at(x, k, nx)
        return rc(mixed.at[to], obuf.at[owner], o_ss.at[k - 1], o_rs.at[k - 1], x=to)

    order_x = (*far_first(nx), 0)
    rec = jnp.concatenate([xrec[i] for i in range(nx)], axis=1)
    parts[...] = (pacc[...] + nt(rec, wor[...])).astype(BF16).reshape(nx, 2, HALF, cols_out)
    for k in order_x:
        to_half(at(x, k, nx)).start()
    for k in order_x:
        s = at(x, k, nx)
        to_half(s).wait_recv()
        joint = (parts[s, c].astype(F32) + part_in[s].astype(F32)).astype(BF16)
        if k:
            mixed[s] = joint
            deliver(k, x).start()
        else:
            obuf[x] = joint
    for k in range(1, nx):
        deliver(k, at(x, -k, nx)).wait_recv()

    chunk = min(HEAD, cols_out)
    total_cols = chunk * nx
    src = lax.broadcasted_iota(jnp.int32, (total_cols, total_cols), 0)
    dst = lax.broadcasted_iota(jnp.int32, (total_cols, total_cols), 1)
    wanted = (
        lax.div(lax.rem(dst, 32), wo_cols) * chunk
        + lax.div(dst, 32) * wo_cols
        + lax.rem(dst, wo_cols)
    )
    order = (src == wanted).astype(BF16)
    for q in range(cols_out // chunk):
        cols = slice(q * chunk, (q + 1) * chunk)
        joined = jnp.concatenate([obuf[i, :, cols] for i in range(nx)], axis=1)
        out_ref[0, :, q * total_cols : (q + 1) * total_cols] = nn(joined, order).astype(BF16)

    for st in range(3):
        p1_done(st)
        p2_done(st)
    tokens.done()
    pool_ring.done()
    rec_ring.done()
    for slot, owner in enumerate((x, left, right, across)):
        to_partner(slot, owner, c).wait_send()
    for k in range(1, nx):
        spikes(k, x).wait_send()
        deliver(k, x).wait_send()
    for k in range(1, ny):
        c1(k, y).wait_send()
        c3(k, y).wait_send()
    if nz > 1:

        def sent_later(k, _):
            c2(k, z, z + k).wait_send()
            return _

        lax.fori_loop(1, nz - z, sent_later, 0)
    for s in range(nx):
        to_half(s).wait_send()

    @pl.when(sp < last)
    def _():
        halo_copy(c=1 - c).wait_send()


def body(sizes, *arrays):
    nz, ny, nx = sizes
    (tok, gin, wp, wq, wf, wv, maps, scale, lb, spike, hg, wpo, wro) = arrays
    width = tok.shape[2]
    rows = nx * TOK
    piece = HEAD // ny
    packed = nx * piece
    wo_cols = 32 // nx
    cols_out = nz * ny * wo_cols
    kdim = nx * HEAD
    ring = [pltpu.SemaphoreType.DMA((6,))] * 2
    ring_inputs = [
        pltpu.VMEM(tok.shape, BF16),
        pltpu.VMEM((1, width), F32),
        pltpu.VMEM(maps.shape, BF16),
        pltpu.VMEM((1, kdim), F32),
        pltpu.VMEM((nx, HEAD), F32),
        pltpu.VMEM((1, spike.shape[2], TOK), F32),
        pltpu.VMEM((nx, HEAD), F32),
        pltpu.VMEM((2, 32, kdim), BF16),
    ]
    scratch = [
        *ring_inputs,
        pltpu.VMEM((nx, 2, HALF, width), BF16),
        pltpu.VMEM((3, nz, ny, 2, WROWS, WCOLS), BF16),
        pltpu.VMEM((2, 32, kdim), F32),
        pltpu.VMEM((cols_out, kdim), BF16),
        pltpu.VMEM((cols_out, kdim), BF16),
        pltpu.VMEM((nx, spike.shape[2], TOK), F32),
        pltpu.VMEM((rows, HEAD), BF16),
        pltpu.VMEM((rows, HEAD), BF16),
        pltpu.VMEM((rows, HEAD), BF16),
        pltpu.VMEM((nx, TOK, HEAD), BF16),
        pltpu.VMEM((rows, HEAD), F32),
        pltpu.VMEM((rows, HEAD), F32),
        pltpu.VMEM((ny, packed + 16, HEAD), BF16),
        pltpu.VMEM((ny, packed + 16, HEAD), BF16),
        pltpu.VMEM((ny, packed, HEAD), F32),
        pltpu.VMEM((ny, 8, HEAD), F32),
        pltpu.VMEM((packed + 16, HEAD), BF16),
        pltpu.VMEM((nz, packed + 16, HEAD), BF16),
        pltpu.VMEM((ny, packed, HEAD), BF16),
        pltpu.VMEM((ny, packed, HEAD), BF16),
        pltpu.VMEM((nx, HALO, HEAD), BF16),
        pltpu.VMEM((rows, HEAD), F32),
        pltpu.VMEM((nx, rows, HEAD), BF16),
        pltpu.VMEM((nx, rows, HEAD), BF16),
        pltpu.VMEM((rows, cols_out), F32),
        pltpu.VMEM((nx, 2, HALF, cols_out), BF16),
        pltpu.VMEM((nx, HALF, cols_out), BF16),
        pltpu.VMEM((nx, HALF, cols_out), BF16),
        pltpu.VMEM((nx, HALF, cols_out), BF16),
        *[pltpu.SemaphoreType.DMA((3, 2, max(nz, ny) - 1))] * 2,
        *[pltpu.SemaphoreType.DMA((3, 2, 2, 4, PARTS))] * 2,
        *ring,
        *[pltpu.SemaphoreType.DMA((nx,))] * 2,
        *[pltpu.SemaphoreType.DMA((nx - 1,))] * 2,
        *[pltpu.SemaphoreType.DMA((max(ny - 1, 1),))] * 2,
        *[pltpu.SemaphoreType.DMA((max(nz - 1, 1),))] * 2,
        *[pltpu.SemaphoreType.DMA((max(ny - 1, 1),))] * 2,
        *[pltpu.SemaphoreType.DMA] * 2,
        *ring,
        *ring,
        *[pltpu.SemaphoreType.DMA((nx,))] * 2,
        *[pltpu.SemaphoreType.DMA((nx - 1,))] * 2,
        pltpu.SemaphoreType.DMA((17,)),
    ]
    return pl.pallas_call(
        functools.partial(kernel, sizes),
        out_shape=jax.ShapeDtypeStruct(tok.shape, BF16),
        in_specs=[pl.BlockSpec(memory_space=pltpu.HBM)] * 13,
        out_specs=pl.BlockSpec(memory_space=pltpu.VMEM),
        scratch_shapes=scratch,
        compiler_params=pltpu.CompilerParams(
            collective_id=0, has_side_effects=True, vmem_limit_bytes=56 * 1024 * 1024
        ),
        name="layer",
    )(
        tok,
        gin.reshape(1, width),
        wp,
        wq,
        wf,
        wv,
        maps,
        scale.reshape(1, kdim),
        lb.reshape(nx, HEAD),
        jnp.swapaxes(spike, 1, 2),
        hg.reshape(nx, HEAD),
        wpo.T,
        wro.T,
    )


def layout(devices, sizes):
    nz, ny, nx = sizes
    torus = Mesh(devices.reshape(nz, ny, nx, 2), ("z", "y", "x", "c"))
    sp = ("z", "y")
    return jax.shard_map(
        functools.partial(body, sizes),
        mesh=torus,
        in_specs=(
            P("x", ("z", "y", "c"), None),
            P(),
            P(sp, "c"),
            P(sp, "c"),
            P(sp, "c"),
            P(sp, "c"),
            P("c", None, None),
            P("c"),
            P("c"),
            P("x", sp, "c"),
            P("c"),
            P("c", sp),
            P("c", sp),
        ),
        out_specs=P("x", ("z", "y", "c"), None),
        check_vma=False,
    )


def solution(mesh):
    return layout(mesh.devices, (8, 8, mesh.shape["fs"]))
```

```python
import functools

import jax
import jax.numpy as jnp
from jax import lax
from jax.experimental import pallas as pl
from jax.experimental.pallas import tpu as pltpu
from jax.sharding import Mesh
from jax.sharding import PartitionSpec as P

MESH = pl.DeviceIdType.MESH
BLOCK = 64
HEAD = 128
TOK = 128
HALF = 64
WROWS = 16
WCOLS = 256
HALO = 16
PARTS = 2
EPS = 1e-06
F32 = jnp.float32
BF16 = jnp.bfloat16


def three_parts(value):
    high = value.astype(BF16)
    rest = value - high.astype(F32)
    mid = rest.astype(BF16)
    low = (rest - mid.astype(F32)).astype(BF16)
    return high, mid, low


def nt(a, b):
    return lax.dot_general(a, b, (((1,), (1,)), ((), ())), preferred_element_type=F32)


def tn(a, b):
    return lax.dot_general(a, b, (((0,), (0,)), ((), ())), preferred_element_type=F32)


def nn(a, b):
    return jnp.dot(a, b, preferred_element_type=F32)


def kernel(
    sizes,
    tok_hbm,
    gin_hbm,
    wp_hbm,
    wq_hbm,
    wf_hbm,
    wv_hbm,
    maps_hbm,
    scale_hbm,
    lb_hbm,
    spike_hbm,
    hg_hbm,
    wpo_hbm,
    wro_hbm,
    out_ref,
    tok_ref,
    gin_ref,
    maps_ref,
    scale_ref,
    lb_ref,
    spike_ref,
    hg_ref,
    wo_ref,
    tokbuf,
    wbuf,
    wqp,
    wobuf,
    wop,
    wor,
    spbuf,
    fbuf,
    vbuf,
    qbuf,
    pbuf,
    cfull,
    inner_buf,
    c1_send,
    c1_recv,
    pex,
    dex,
    c2_send,
    c2_recv,
    c3_send,
    c3_recv,
    halo,
    within,
    xpool,
    xrec,
    pacc,
    parts,
    part_in,
    mixed,
    obuf,
    p1_ss,
    p1_rs,
    p2_ss,
    p2_near,
    p2_rest,
    tok_ss,
    tok_rs,
    d2d_ss,
    d2d_rs,
    sp_ss,
    sp_rs,
    c1_ss,
    c1_rs,
    c2_ss,
    c2_rs,
    c3_ss,
    c3_rs,
    halo_ss,
    halo_rs,
    xp_ss,
    xp_rs,
    xr_ss,
    xr_rs,
    part_ss,
    part_rs,
    o_ss,
    o_rs,
    in_sems,
):
    nz, ny, nx = sizes
    z, y, x, c = (lax.axis_index(name) for name in ("z", "y", "x", "c"))
    sp = z * ny + y
    width = tok_hbm.shape[2]
    wo_cols = 32 // nx
    piece = HEAD // ny
    packed = nx * piece
    half_pool = nx * HEAD

    def rc(src, dst, ss, rs, **device):
        return pltpu.make_async_remote_copy(
            src_ref=src, dst_ref=dst, send_sem=ss, recv_sem=rs, device_id=device, device_id_type=MESH
        )

    def taken(sem, ref):
        rc(ref, ref, sp_ss, sem, c=1 - c).wait_recv()

    def left_here(sem, ref):
        rc(ref, ref, sem, sp_rs, c=1 - c).wait_send()

    def far_first(count):
        return sorted(range(1, count), key=lambda k: -min(k, count - k))

    def at(base, step, count):
        return lax.rem(base + step + count, count)

    pltpu.make_async_copy(tok_hbm, tok_ref, in_sems.at[0]).start()
    lanes = pl.ds(pl.multiple_of(x * HEAD, HEAD), HEAD)
    slices = []
    for n, ref in enumerate((wf_hbm, wv_hbm)):
        for p in range(2):
            slices.append(
                pltpu.make_async_copy(
                    ref.at[p * WROWS : (p + 1) * WROWS, lanes],
                    wbuf.at[0, z, y, p, :, pl.ds(n * HEAD, HEAD)],
                    in_sems.at[1],
                )
            )
    for n, ref in enumerate((wq_hbm, wp_hbm)):
        slices.append(
            pltpu.make_async_copy(ref.at[:, lanes], wqp.at[n, z, y], in_sems.at[2])
        )
    def fetched(n):
        pltpu.make_async_copy(wbuf.at[0, z, y], wbuf.at[0, z, y], in_sems.at[n]).wait()

    small = [
        pltpu.make_async_copy(src, dst, in_sems.at[3 + min(n, 2) if n < 4 else n + 2])
        for n, (src, dst) in enumerate(
            (
                (gin_hbm, gin_ref),
                (spike_hbm, spike_ref),
                (wpo_hbm, wo_ref.at[0]),
                (wro_hbm, wo_ref.at[1]),
                (lb_hbm, lb_ref),
                (hg_hbm, hg_ref),
                (scale_hbm, scale_ref),
                (maps_hbm, maps_ref),
            )
        )
    ]
    for copy in slices[:4] + small[:2] + slices[4:] + small[2:]:
        copy.start()

    barrier = pltpu.get_barrier_semaphore()

    def greet(**device):
        pl.semaphore_signal(barrier, inc=1, device_id=device, device_id_type=MESH)

    for k in range(1, ny):
        greet(y=at(y, k, ny))
    for k in range(1, nz):
        greet(z=at(z, k, nz))
    for k in range(1, nx):
        greet(x=at(x, k, nx))
    greet(c=1 - c)
    if nz > 1 and ny > 1:
        down = jnp.logical_and(y == ny - 1, z < nz - 1)
        up = jnp.logical_and(y == 0, z > 0)

        @pl.when(down)
        def _():
            greet(z=z + 1, y=0)

        @pl.when(up)
        def _():
            greet(z=z - 1, y=ny - 1)

    greeted = (ny - 1) + (nz - 1) + (nx - 1) + 1
    if nz > 1 and ny > 1:
        at_end = (y // (ny - 1)) * (1 - z // (nz - 1))
        at_start = ((ny - 1 - y) // (ny - 1)) * (1 - (nz - 1 - z) // (nz - 1))
        greeted = greeted + at_end + at_start
    fetched(1)
    pl.semaphore_wait(barrier, greeted)

    def wslot(st, path, zz, yy):
        return wqp.at[path, zz, yy] if st == 1 else wbuf.at[st // 2, zz, yy, path]

    def p1(st, k, path):
        if path == 0:
            return lambda zz, zt: rc(
                wslot(st, 0, zz, y),
                wslot(st, 0, zz, y),
                p1_ss.at[st],
                p1_rs.at[st],
                z=zt,
            )
        return lambda yy, yt: rc(
            wslot(st, 1, z, yy),
            wslot(st, 1, z, yy),
            p1_ss.at[st],
            p1_rs.at[st],
            y=yt,
        )

    def p1_send(st):
        for k in far_first(max(nz, ny)):
            if k < nz:
                p1(st, k, 0)(z, at(z, k, nz)).start()
            if k < ny:
                p1(st, k, 1)(y, at(y, k, ny)).start()

    def p1_wait(st):
        taken(p1_rs.at[st], wbuf.at[0, 0, 0 : ny - 1])

    def p1_done(st):
        left_here(p1_ss.at[st], wbuf.at[0, 0, 0 : ny - 1])

    paths = ((0, ny, nz), (1, nz, ny))

    def p2(st, path, way, source, distance, part):
        sign = 1 if way == 0 else -1
        if path == 0:
            size = nz // PARTS
            block = wslot(st, 0, pl.ds(part * size, size), at(y, -sign * source, ny))
            device = {"y": at(y, sign * max(distance - source, 1), ny)}
        else:
            size = ny // PARTS
            block = wslot(st, 1, at(z, -sign * source, nz), pl.ds(part * size, size))
            device = {"z": at(z, sign * max(distance - source, 1), nz)}
        arrives = p2_near.at[st, part] if distance == 2 else p2_rest.at[st, path]
        return rc(block, block, p2_ss.at[st], arrives, **device)

    def far_way(part):
        return 0 if part < PARTS // 2 else 1

    def each(part):
        return [(path, way, part) for path in range(2) for way in range(2)]

    def p2_own(st):
        for part in range(PARTS):
            for distance in (2, 1):
                for path, way, _ in each(part):
                    p2(st, path, way, 0, distance, part).start()

    def p2_relay(st):
        for part in range(PARTS):
            taken(p2_near.at[st, part], wbuf.at[0, 0, 0 : 2 * ny // PARTS])
            for path, way, _ in each(part):
                if way == far_way(part):
                    p2(st, path, way, 2, 4, part).start()
                p2(st, path, way, 2, 3, part).start()

    def p2_wait(st, only=(0, 1)):
        for path in only:
            taken(p2_rest.at[st, path], wbuf.at[0, 0:5, 0 : ny // 2])

    def p2_done(st):
        left_here(p2_ss.at[st], wbuf.at[0, 0 : nz - 1])

    right, left, across = at(x, 1, nx), at(x, -1, nx), at(x, 2, nx)

    def token_half(kind, owner, half, to):
        ref = tokbuf.at[owner, c, pl.ds(half * (HALF // 2), HALF // 2)]
        return rc(ref, ref, tok_ss, tok_rs.at[kind], x=to)

    def tokens_start():
        token_half(0, x, 0, right).start()
        token_half(1, x, 1, left).start()
        token_half(2, x, 1, right).start()
        token_half(2, x, 0, left).start()

    def tokens_forward():
        token_half(0, left, 0, right).wait_recv()
        token_half(3, left, 0, right).start()
        token_half(1, right, 1, left).wait_recv()
        token_half(3, right, 1, left).start()

    def tokens_near():
        taken(tok_rs.at[2], tokbuf.at[0, 0])

    def tokens_far():
        taken(tok_rs.at[3], tokbuf.at[0, 0])

    def to_all_x(ref_of, ss, rs):
        for k in (2, 1, 3):
            rc(ref_of(x), ref_of(x), ss, rs, x=at(x, k, nx)).start()

    def to_partner(owner, core):
        return rc(
            tokbuf.at[owner, core], tokbuf.at[owner, core], d2d_ss, d2d_rs, c=1 - c
        )

    def spikes(k, owner):
        return rc(spbuf.at[owner], spbuf.at[owner], sp_ss, sp_rs, x=at(x, k, nx))

    p1_send(0)
    pltpu.make_async_copy(tok_hbm, tok_ref, in_sems.at[0]).wait()
    small[0].wait()
    own = tok_ref[0].astype(F32)
    square = jnp.mean(own * own, axis=-1, keepdims=True)
    tokbuf[x, c] = (own * lax.rsqrt(square + EPS) * gin_ref[...]).astype(BF16)
    small[1].wait()
    spbuf[x] = spike_ref[0]
    fetched(2)
    tokens_start()
    to_partner(x, c).start()
    for k in range(1, nx):
        spikes(k, x).start()
    p1_send(1)

    pltpu.make_async_copy(wo_ref, wo_ref, in_sems.at[5]).wait()
    for copy in small[4:]:
        copy.wait()
    wobuf[...] = wo_ref[...].astype(F32)
    mine = pl.ds(pl.multiple_of(x * wo_cols, wo_cols), wo_cols)
    block = jnp.concatenate([wobuf[0, mine, :], wobuf[1, mine, :]], axis=0).astype(BF16)
    for p in range(2):
        wbuf[1, z, y, p] = block[:, p * WCOLS : (p + 1) * WCOLS]

    p1_wait(0)
    p2_own(0)
    tokens_forward()
    tokens_near()
    to_partner(left, c).start()
    to_partner(right, c).start()
    p2_relay(0)
    p1_wait(1)
    p2_own(1)
    p1_send(2)
    tokens_far()
    to_partner(across, c).start()
    taken(d2d_rs, tokbuf.at[:, 0])
    taken(sp_rs, spbuf.at[0 : nx - 1])
    p2_wait(0)

    rows = nx * TOK

    def project(weights):
        return nn(tokbuf[...].reshape(rows, width), weights).astype(BF16)

    projected = project(wbuf[0].reshape(width, WCOLS))
    fbuf[...] = projected[:, :HEAD]
    vbuf[...] = projected[:, HEAD:]

    ti = lax.broadcasted_iota(jnp.int32, (TOK, TOK), 0)
    si = lax.broadcasted_iota(jnp.int32, (TOK, TOK), 1)
    same = (ti // BLOCK) == (si // BLOCK)
    causal = jnp.logical_and(same, ti >= si)
    lower = causal.astype(F32)
    lower_b = lower.astype(BF16)
    ones_b = jnp.ones((TOK, HEAD), BF16)
    second = lax.broadcasted_iota(jnp.int32, (TOK, HEAD), 0) >= BLOCK
    lb_gate = 1.0 / (1.0 + jnp.exp(lb_ref[pl.ds(x, 1), :]))
    keys = lb_gate * (1.0 / (1.0 + jnp.exp(fbuf[...].astype(F32))))
    logs = three_parts(jnp.log(1.0 - keys))
    inners = []
    for s in range(nx):
        span = slice(s * TOK, (s + 1) * TOK)
        spread = three_parts(lower * spbuf[s, pl.ds(x, 1), :])
        inners.append(
            nn(
                jnp.concatenate([lower_b, lower_b, lower_b, *spread], axis=1),
                jnp.concatenate([*(part[span] for part in logs), ones_b, ones_b, ones_b], axis=0),
            )
        )
    decays, tails = [], []
    for s in range(nx):
        span = slice(s * TOK, (s + 1) * TOK)
        inner = inners[s]
        first_end = inner[BLOCK - 1 : BLOCK, :]
        total = first_end + inner[TOK - 1 : TOK, :]
        full = inner + jnp.where(second, first_end, 0.0)
        inner_buf[span, :] = inner
        cfull[span, :] = full
        tails.append((keys[span] * jnp.exp(total - full)).astype(BF16))
        decays.append(jnp.exp(total))
    for s in range(nx):
        state = tn(vbuf[s * TOK : (s + 1) * TOK, :], tails[s]).astype(BF16)
        for j in range(ny):
            c1_send[j, s * piece : (s + 1) * piece, :] = state[j * piece : (j + 1) * piece, :]

    def decay_rows(values):
        out = []
        for value in values:
            high = value.astype(BF16).astype(F32)
            out += [high, value - high]
        out.append(jnp.zeros((16 - len(out), HEAD), F32))
        return jnp.concatenate(out, axis=0).astype(BF16)

    extra = decay_rows(decays)
    for j in range(ny):
        c1_send[j, packed : packed + 16, :] = extra
    c1_recv[y] = c1_send[y]

    def c1(k, slot):
        to = at(y, k, ny)
        return rc(c1_send.at[to], c1_recv.at[slot], c1_ss, c1_rs, y=to)

    for k in far_first(ny):
        c1(k, y).start()

    p2_relay(1)

    taken(c1_rs, c1_send.at[0 : ny - 1])

    def read_decay(block, s):
        at_row = packed + 2 * s
        return block[at_row : at_row + 1, :] + block[at_row + 1 : at_row + 2, :]

    run = [jnp.zeros((piece, HEAD), F32) for _ in range(nx)]
    fade = [jnp.ones((1, HEAD), F32) for _ in range(nx)]
    for j in range(ny):
        block = c1_recv[j].astype(F32)
        for s in range(nx):
            pex[j, s * piece : (s + 1) * piece, :] = run[s]
            dex[j, s : s + 1, :] = fade[s]
            decay = read_decay(block, s)
            run[s] = decay * run[s] + block[s * piece : (s + 1) * piece, :]
            fade[s] = fade[s] * decay
    c2_send[0:packed, :] = jnp.concatenate(run, axis=0).astype(BF16)
    c2_send[packed : packed + 16, :] = decay_rows(fade)

    def c2(k, slot, to):
        return rc(c2_send, c2_recv.at[slot], c2_ss.at[k - 1], c2_rs.at[k - 1], z=to)

    if nz > 1:

        def send_later(k, _):
            c2(k, z, z + k).start()
            return _

        lax.fori_loop(1, nz - z, send_later, 0)

    p1_wait(2)
    p2_own(2)
    p2_wait(1, (1,))
    pbuf[...] = project(wqp[1].reshape(width, HEAD)).reshape(nx, TOK, HEAD)

    last = nz * ny - 1
    halo_src = pbuf.at[:, TOK - HALO : TOK]

    def halo_copy(**device):
        return rc(halo_src, halo, halo_ss, halo_rs, **device)

    if ny > 1:

        @pl.when(y < ny - 1)
        def _():
            halo_copy(y=y + 1).start()

    if nz > 1:

        @pl.when(jnp.logical_and(y == ny - 1, z < nz - 1))
        def _():
            halo_copy(z=z + 1, y=0).start()

    @pl.when(sp == 0)
    def _():
        halo[...] = jnp.zeros_like(halo)

    p2_wait(1, (0,))
    qbuf[...] = project(wqp[0].reshape(width, HEAD))

    for s in range(nx):
        span = slice(s * TOK, (s + 1) * TOK)
        query = qbuf[span, :].astype(F32)
        reader = query * (1.0 / (1.0 + jnp.exp(-query)))
        key = lb_gate * (1.0 / (1.0 + jnp.exp(fbuf[span, :].astype(F32))))
        inner = inner_buf[span, :]
        scaled = (reader * jnp.exp(inner)).astype(BF16)
        near = (key * jnp.exp(-inner)).astype(BF16)
        tail = (
            key[:BLOCK] * jnp.exp(inner[BLOCK - 1 : BLOCK, :] - inner[:BLOCK])
        ).astype(BF16)
        scores = nt(scaled, jnp.concatenate([near, tail], axis=0))
        cross = jnp.concatenate([scores[:, TOK:], scores[:, TOK:]], axis=1)
        before = jnp.logical_and(ti >= BLOCK, si < BLOCK)
        chosen = jnp.where(causal, scores[:, :TOK], jnp.where(before, cross, 0.0))
        within[span, :] = nn(chosen.astype(BF16), vbuf[span, :])
        cfull[span, :] = reader * jnp.exp(cfull[span, :])
    if ny > 1:

        @pl.when(y > 0)
        def _():
            halo_copy(y=y - 1).wait_recv()

    if nz > 1:

        @pl.when(jnp.logical_and(y == 0, z > 0))
        def _():
            halo_copy(z=z - 1, y=ny - 1).wait_recv()

    group = (c * half_pool + x * HEAD) // WCOLS
    window = jnp.where(group == 0, 2, jnp.where(group == 1, 4, jnp.where(group == 2, 8, 16)))
    band = jnp.logical_and(ti >= si, ti - si < window).astype(BF16)
    hi = lax.broadcasted_iota(jnp.int32, (TOK, HALO), 0)
    hj = lax.broadcasted_iota(jnp.int32, (TOK, HALO), 1)
    band_before = (hi + HALO - hj < window).astype(BF16)
    place = sp * TOK + lax.broadcasted_iota(jnp.int32, (TOK, HEAD), 0) + 1
    count = jnp.minimum(place, window).astype(F32)
    for s in range(nx):
        sums = nn(band, pbuf[s]) + nn(band_before, halo[s])
        xpool[x, s * TOK : (s + 1) * TOK, :] = (sums / count - pbuf[s].astype(F32)).astype(BF16)

    to_all_x(lambda owner: xpool.at[owner], xp_ss, xp_rs)

    def add_row(zz, carry):
        if nz > 1:
            rc(
                c2_send, c2_recv.at[zz], c2_ss.at[z - zz - 1], c2_rs.at[z - zz - 1], z=zz
            ).wait_recv()
        block = c2_recv[zz].astype(F32)
        out = []
        for s in range(nx):
            out.append(
                read_decay(block, s) * carry[s] + block[s * piece : (s + 1) * piece, :]
            )
        return tuple(out)

    earlier = tuple(jnp.zeros((piece, HEAD), F32) for _ in range(nx))
    if nz > 1:
        earlier = lax.fori_loop(0, z, add_row, earlier)
    for j in range(ny):
        for s in range(nx):
            span = slice(s * piece, (s + 1) * piece)
            c3_send[j, span, :] = (dex[j, s : s + 1, :] * earlier[s] + pex[j, span, :]).astype(BF16)
    c3_recv[y] = c3_send[y]

    def c3(k, slot):
        to = at(y, k, ny)
        return rc(c3_send.at[to], c3_recv.at[slot], c3_ss, c3_rs, y=to)

    for k in far_first(ny):
        c3(k, y).start()

    p2_relay(2)
    taken(c3_rs, c3_send.at[0 : ny - 1])
    gain = hg_ref[pl.ds(x, 1), :]

    def finish(s):
        span = slice(s * TOK, (s + 1) * TOK)
        prior = c3_recv[:, s * piece : (s + 1) * piece, :].reshape(HEAD, HEAD)
        read = within[span, :] + nt(cfull[span, :].astype(BF16), prior)
        square = jnp.mean(read * read, axis=-1, keepdims=True)
        normal = (read * lax.rsqrt(square + EPS) * gain).astype(BF16)
        xrec[x, s] = normal.reshape(2, HALF, HEAD)

    for s in range(nx):
        finish(s)
    to_all_x(lambda owner: xrec.at[owner], xr_ss, xr_rs)
    taken(xp_rs, xpool.at[0 : nx - 1])
    pieces = []
    for g in range(half_pool // WCOLS):
        cols = slice(g * WCOLS, (g + 1) * WCOLS)
        diff = jnp.concatenate([xpool[2 * g], xpool[2 * g + 1]], axis=1)
        pieces.append((nn(diff, maps_ref[g]) * scale_ref[:, cols]).astype(BF16))
    p2_wait(2)
    for p in range(2):
        both = wbuf[1, :, :, p].reshape(nz * ny, 2 * wo_cols, WCOLS).astype(F32)
        cols = slice(p * WCOLS, (p + 1) * WCOLS)
        wop[:, cols] = both[:, :wo_cols].reshape(nz * ny * wo_cols, WCOLS).astype(BF16)
        wor[:, cols] = both[:, wo_cols:].reshape(nz * ny * wo_cols, WCOLS).astype(BF16)
    pooled_out = nt(jnp.concatenate(pieces, axis=1), wop[...])
    pacc[...] = pooled_out.reshape(nx, 2, HALF, nz * ny * wo_cols)
    taken(xr_rs, xrec.at[0 : nx - 1])
    cols_out = nz * ny * wo_cols

    def to_half(s):
        return rc(parts.at[s, 1 - c], part_in.at[s], part_ss, part_rs.at[s], c=1 - c)

    def deliver(k, owner):
        to = at(x, k, nx)
        return rc(mixed.at[to], obuf.at[owner], o_ss, o_rs, x=to)

    order_x = (*far_first(nx), 0)
    def half_of(core):
        rec = jnp.concatenate([xrec[i, :, core].reshape(nx * HALF, HEAD) for i in range(nx)], axis=1)
        pooled = pacc[:, core].reshape(nx * HALF, cols_out)
        parts[:, core] = (pooled + nt(rec, wor[...])).astype(BF16).reshape(nx, HALF, cols_out)

    half_of(1 - c)
    for k in order_x:
        to_half(at(x, k, nx)).start()
    half_of(c)
    for k in order_x:
        s = at(x, k, nx)
        to_half(s).wait_recv()
        joint = (parts[s, c].astype(F32) + part_in[s].astype(F32)).astype(BF16)
        if k:
            mixed[s] = joint
            deliver(k, x).start()
        else:
            obuf[x] = joint
    taken(o_rs, mixed.at[0 : nx - 1])

    chunk = min(HEAD, cols_out)
    total_cols = chunk * nx
    src = lax.broadcasted_iota(jnp.int32, (total_cols, total_cols), 0)
    dst = lax.broadcasted_iota(jnp.int32, (total_cols, total_cols), 1)
    wanted = (
        lax.div(lax.rem(dst, 32), wo_cols) * chunk
        + lax.div(dst, 32) * wo_cols
        + lax.rem(dst, wo_cols)
    )
    order = (src == wanted).astype(BF16)
    for q in range(cols_out // chunk):
        cols = slice(q * chunk, (q + 1) * chunk)
        joined = jnp.concatenate([obuf[i, :, cols] for i in range(nx)], axis=1)
        out_ref[0, :, q * total_cols : (q + 1) * total_cols] = nn(joined, order).astype(BF16)

    for st in range(3):
        p1_done(st)
        p2_done(st)
    left_here(tok_ss, tokbuf.at[0:3, 0])
    left_here(d2d_ss, tokbuf.at[:, 0])
    left_here(sp_ss, spbuf.at[0 : nx - 1])
    left_here(c1_ss, c1_send.at[0 : ny - 1])
    left_here(c3_ss, c3_send.at[0 : ny - 1])
    left_here(xp_ss, xpool.at[0 : nx - 1])
    left_here(xr_ss, xrec.at[0 : nx - 1])
    left_here(o_ss, mixed.at[0 : nx - 1])
    left_here(part_ss, part_in)
    if nz > 1:

        def sent_later(k, _):
            c2(k, z, z + k).wait_send()
            return _

        lax.fori_loop(1, nz - z, sent_later, 0)
    @pl.when(sp < last)
    def _():
        halo_copy(c=1 - c).wait_send()


def body(sizes, *arrays):
    nz, ny, nx = sizes
    (tok, gin, wp, wq, wf, wv, maps, scale, lb, spike, hg, wpo, wro) = arrays
    width = tok.shape[2]
    rows = nx * TOK
    piece = HEAD // ny
    packed = nx * piece
    wo_cols = 32 // nx
    cols_out = nz * ny * wo_cols
    kdim = nx * HEAD
    ring_inputs = [
        pltpu.VMEM(tok.shape, BF16),
        pltpu.VMEM((1, width), F32),
        pltpu.VMEM(maps.shape, BF16),
        pltpu.VMEM((1, kdim), F32),
        pltpu.VMEM((nx, HEAD), F32),
        pltpu.VMEM((1, spike.shape[2], TOK), F32),
        pltpu.VMEM((nx, HEAD), F32),
        pltpu.VMEM((2, 32, kdim), BF16),
    ]
    scratch = [
        *ring_inputs,
        pltpu.VMEM((nx, 2, HALF, width), BF16),
        pltpu.VMEM((2, nz, ny, 2, WROWS, WCOLS), BF16),
        pltpu.VMEM((2, nz, ny, 2 * WROWS, HEAD), BF16),
        pltpu.VMEM((2, 32, kdim), F32),
        pltpu.VMEM((cols_out, kdim), BF16),
        pltpu.VMEM((cols_out, kdim), BF16),
        pltpu.VMEM((nx, spike.shape[2], TOK), F32),
        pltpu.VMEM((rows, HEAD), BF16),
        pltpu.VMEM((rows, HEAD), BF16),
        pltpu.VMEM((rows, HEAD), BF16),
        pltpu.VMEM((nx, TOK, HEAD), BF16),
        pltpu.VMEM((rows, HEAD), F32),
        pltpu.VMEM((rows, HEAD), F32),
        pltpu.VMEM((ny, packed + 16, HEAD), BF16),
        pltpu.VMEM((ny, packed + 16, HEAD), BF16),
        pltpu.VMEM((ny, packed, HEAD), F32),
        pltpu.VMEM((ny, 8, HEAD), F32),
        pltpu.VMEM((packed + 16, HEAD), BF16),
        pltpu.VMEM((nz, packed + 16, HEAD), BF16),
        pltpu.VMEM((ny, packed, HEAD), BF16),
        pltpu.VMEM((ny, packed, HEAD), BF16),
        pltpu.VMEM((nx, HALO, HEAD), BF16),
        pltpu.VMEM((rows, HEAD), F32),
        pltpu.VMEM((nx, rows, HEAD), BF16),
        pltpu.VMEM((nx, nx, 2, HALF, HEAD), BF16),
        pltpu.VMEM((nx, 2, HALF, cols_out), F32),
        pltpu.VMEM((nx, 2, HALF, cols_out), BF16),
        pltpu.VMEM((nx, HALF, cols_out), BF16),
        pltpu.VMEM((nx, HALF, cols_out), BF16),
        pltpu.VMEM((nx, HALF, cols_out), BF16),
        *[pltpu.SemaphoreType.DMA((3,))] * 2,
        pltpu.SemaphoreType.DMA((3,)),
        pltpu.SemaphoreType.DMA((3, PARTS)),
        pltpu.SemaphoreType.DMA((3, 2)),
        pltpu.SemaphoreType.DMA,
        pltpu.SemaphoreType.DMA((4,)),
        *[pltpu.SemaphoreType.DMA] * 2,
        *[pltpu.SemaphoreType.DMA] * 2,
        *[pltpu.SemaphoreType.DMA] * 2,
        *[pltpu.SemaphoreType.DMA((max(nz - 1, 1),))] * 2,
        *[pltpu.SemaphoreType.DMA] * 2,
        *[pltpu.SemaphoreType.DMA] * 2,
        *[pltpu.SemaphoreType.DMA] * 2,
        *[pltpu.SemaphoreType.DMA] * 2,
        pltpu.SemaphoreType.DMA,
        pltpu.SemaphoreType.DMA((nx,)),
        *[pltpu.SemaphoreType.DMA] * 2,
        pltpu.SemaphoreType.DMA((10,)),
    ]
    return pl.pallas_call(
        functools.partial(kernel, sizes),
        out_shape=jax.ShapeDtypeStruct(tok.shape, BF16),
        in_specs=[pl.BlockSpec(memory_space=pltpu.HBM)] * 13,
        out_specs=pl.BlockSpec(memory_space=pltpu.VMEM),
        scratch_shapes=scratch,
        compiler_params=pltpu.CompilerParams(
            collective_id=0, has_side_effects=True, vmem_limit_bytes=56 * 1024 * 1024
        ),
        name="layer",
    )(
        tok,
        gin.reshape(1, width),
        wp,
        wq,
        wf,
        wv,
        maps,
        scale.reshape(1, kdim),
        lb.reshape(nx, HEAD),
        jnp.swapaxes(spike, 1, 2),
        hg.reshape(nx, HEAD),
        wpo.T,
        wro.T,
    )


def layout(devices, sizes):
    nz, ny, nx = sizes
    torus = Mesh(devices.reshape(nz, ny, nx, 2), ("z", "y", "x", "c"))
    sp = ("z", "y")
    return jax.shard_map(
        functools.partial(body, sizes),
        mesh=torus,
        in_specs=(
            P("x", ("z", "y", "c"), None),
            P(),
            P(sp, "c"),
            P(sp, "c"),
            P(sp, "c"),
            P(sp, "c"),
            P("c", None, None),
            P("c"),
            P("c"),
            P("x", sp, "c"),
            P("c"),
            P("c", sp),
            P("c", sp),
        ),
        out_specs=P("x", ("z", "y", "c"), None),
        check_vma=False,
    )


def solution(mesh):
    return layout(mesh.devices, (8, 8, mesh.shape["fs"]))
```

```python
import functools

import jax
import jax.numpy as jnp
from jax import lax
from jax.experimental import pallas as pl
from jax.experimental.pallas import tpu as pltpu
from jax.sharding import Mesh
from jax.sharding import PartitionSpec as P

MESH = pl.DeviceIdType.MESH
BLOCK = 64
HEAD = 128
TOK = 128
HALF = 64
WROWS = 16
WCOLS = 256
HALO = 16
PARTS = 2
EPS = 1e-06
F32 = jnp.float32
BF16 = jnp.bfloat16


def three_parts(value):
    high = value.astype(BF16)
    rest = value - high.astype(F32)
    mid = rest.astype(BF16)
    low = (rest - mid.astype(F32)).astype(BF16)
    return high, mid, low


def nt(a, b):
    return lax.dot_general(a, b, (((1,), (1,)), ((), ())), preferred_element_type=F32)


def tn(a, b):
    return lax.dot_general(a, b, (((0,), (0,)), ((), ())), preferred_element_type=F32)


def nn(a, b):
    return jnp.dot(a, b, preferred_element_type=F32)


def kernel(
    sizes,
    tok_hbm,
    gin_hbm,
    wp_hbm,
    wq_hbm,
    wf_hbm,
    wv_hbm,
    maps_hbm,
    scale_hbm,
    lb_hbm,
    spike_hbm,
    hg_hbm,
    wpo_hbm,
    wro_hbm,
    out_ref,
    tok_ref,
    gin_ref,
    maps_ref,
    scale_ref,
    lb_ref,
    spike_ref,
    hg_ref,
    wo_ref,
    tokbuf,
    wbuf,
    wqp,
    wobuf,
    wop,
    wor,
    spbuf,
    fbuf,
    vbuf,
    qbuf,
    pbuf,
    cfull,
    inner_buf,
    c1_send,
    c1_recv,
    pex,
    dex,
    c2_send,
    c2_recv,
    c3_send,
    c3_recv,
    halo,
    within,
    xpool,
    xrec,
    pacc,
    parts,
    part_in,
    mixed,
    obuf,
    p1_ss,
    p1_rs,
    p2_ss,
    p2_near,
    p2_rest,
    tok_ss,
    tok_rs,
    d2d_ss,
    d2d_rs,
    sp_ss,
    sp_rs,
    c1_ss,
    c1_rs,
    c2_ss,
    c2_rs,
    c3_ss,
    c3_rs,
    halo_ss,
    halo_rs,
    xp_ss,
    xp_rs,
    xr_ss,
    xr_rs,
    part_ss,
    part_rs,
    o_ss,
    o_rs,
    in_sems,
):
    nz, ny, nx = sizes
    z, y, x, c = (lax.axis_index(name) for name in ("z", "y", "x", "c"))
    sp = z * ny + y
    width = tok_hbm.shape[2]
    wo_cols = 32 // nx
    piece = HEAD // ny
    packed = nx * piece
    half_pool = nx * HEAD

    def rc(src, dst, ss, rs, **device):
        return pltpu.make_async_remote_copy(
            src_ref=src, dst_ref=dst, send_sem=ss, recv_sem=rs, device_id=device, device_id_type=MESH
        )

    def taken(sem, ref):
        rc(ref, ref, sp_ss, sem, c=1 - c).wait_recv()

    def left_here(sem, ref):
        rc(ref, ref, sem, sp_rs, c=1 - c).wait_send()

    def far_first(count):
        return sorted(range(1, count), key=lambda k: -min(k, count - k))

    def at(base, step, count):
        return lax.rem(base + step + count, count)

    pltpu.make_async_copy(tok_hbm, tok_ref, in_sems.at[0]).start()
    lanes = pl.ds(pl.multiple_of(x * HEAD, HEAD), HEAD)
    slices = []
    for n, ref in enumerate((wf_hbm, wv_hbm)):
        for p in range(2):
            slices.append(
                pltpu.make_async_copy(
                    ref.at[p * WROWS : (p + 1) * WROWS, lanes],
                    wbuf.at[0, z, y, p, :, pl.ds(n * HEAD, HEAD)],
                    in_sems.at[1],
                )
            )
    for n, ref in enumerate((wq_hbm, wp_hbm)):
        slices.append(
            pltpu.make_async_copy(ref.at[:, lanes], wqp.at[n, z, y], in_sems.at[2])
        )
    def fetched(n):
        pltpu.make_async_copy(wbuf.at[0, z, y], wbuf.at[0, z, y], in_sems.at[n]).wait()

    small = [
        pltpu.make_async_copy(src, dst, in_sems.at[3 + min(n, 2) if n < 4 else n + 2])
        for n, (src, dst) in enumerate(
            (
                (gin_hbm, gin_ref),
                (spike_hbm, spike_ref),
                (wpo_hbm, wo_ref.at[0]),
                (wro_hbm, wo_ref.at[1]),
                (lb_hbm, lb_ref),
                (hg_hbm, hg_ref),
                (scale_hbm, scale_ref),
                (maps_hbm, maps_ref),
            )
        )
    ]
    for copy in slices[:4] + small[:2] + slices[4:] + small[2:]:
        copy.start()

    barrier = pltpu.get_barrier_semaphore()

    def greet(**device):
        pl.semaphore_signal(barrier, inc=1, device_id=device, device_id_type=MESH)

    for k in range(1, ny):
        greet(y=at(y, k, ny))
    for k in range(1, nz):
        greet(z=at(z, k, nz))
    for k in range(1, nx):
        greet(x=at(x, k, nx))
    greet(c=1 - c)
    if nz > 1 and ny > 1:
        down = jnp.logical_and(y == ny - 1, z < nz - 1)
        up = jnp.logical_and(y == 0, z > 0)

        @pl.when(down)
        def _():
            greet(z=z + 1, y=0)

        @pl.when(up)
        def _():
            greet(z=z - 1, y=ny - 1)

    greeted = (ny - 1) + (nz - 1) + (nx - 1) + 1
    if nz > 1 and ny > 1:
        at_end = (y // (ny - 1)) * (1 - z // (nz - 1))
        at_start = ((ny - 1 - y) // (ny - 1)) * (1 - (nz - 1 - z) // (nz - 1))
        greeted = greeted + at_end + at_start
    fetched(1)
    pl.semaphore_wait(barrier, greeted)

    def wslot(st, path, zz, yy):
        return wqp.at[path, zz, yy] if st == 1 else wbuf.at[st // 2, zz, yy, path]

    def p1(st, k, path):
        if path == 0:
            return lambda zz, zt: rc(
                wslot(st, 0, zz, y),
                wslot(st, 0, zz, y),
                p1_ss.at[st],
                p1_rs.at[st],
                z=zt,
            )
        return lambda yy, yt: rc(
            wslot(st, 1, z, yy),
            wslot(st, 1, z, yy),
            p1_ss.at[st],
            p1_rs.at[st],
            y=yt,
        )

    def p1_send(st):
        for k in far_first(max(nz, ny)):
            if k < nz:
                p1(st, k, 0)(z, at(z, k, nz)).start()
            if k < ny:
                p1(st, k, 1)(y, at(y, k, ny)).start()

    def p1_wait(st):
        taken(p1_rs.at[st], wbuf.at[0, 0, 0 : ny - 1])

    def p1_done(st):
        left_here(p1_ss.at[st], wbuf.at[0, 0, 0 : ny - 1])

    paths = ((0, ny, nz), (1, nz, ny))

    def p2(st, path, way, source, distance, part):
        sign = 1 if way == 0 else -1
        if path == 0:
            size = nz // PARTS
            block = wslot(st, 0, pl.ds(part * size, size), at(y, -sign * source, ny))
            device = {"y": at(y, sign * max(distance - source, 1), ny)}
        else:
            size = ny // PARTS
            block = wslot(st, 1, at(z, -sign * source, nz), pl.ds(part * size, size))
            device = {"z": at(z, sign * max(distance - source, 1), nz)}
        arrives = p2_near.at[st, part] if distance == 2 else p2_rest.at[st, path]
        return rc(block, block, p2_ss.at[st], arrives, **device)

    def far_way(part):
        return 0 if part < PARTS // 2 else 1

    def each(part):
        return [(path, way, part) for path in range(2) for way in range(2)]

    def p2_own(st):
        for part in range(PARTS):
            for distance in (2, 1):
                for path, way, _ in each(part):
                    p2(st, path, way, 0, distance, part).start()

    def p2_relay(st):
        for part in range(PARTS):
            taken(p2_near.at[st, part], wbuf.at[0, 0, 0 : 2 * ny // PARTS])
            for path, way, _ in each(part):
                if way == far_way(part):
                    p2(st, path, way, 2, 4, part).start()
                p2(st, path, way, 2, 3, part).start()

    def p2_wait(st, only=(0, 1)):
        for path in only:
            taken(p2_rest.at[st, path], wbuf.at[0, 0:5, 0 : ny // 2])

    def p2_done(st):
        left_here(p2_ss.at[st], wbuf.at[0, 0 : nz - 1])

    right, left, across = at(x, 1, nx), at(x, -1, nx), at(x, 2, nx)

    def token_half(kind, owner, half, to):
        ref = tokbuf.at[owner, c, pl.ds(half * (HALF // 2), HALF // 2)]
        return rc(ref, ref, tok_ss, tok_rs.at[kind], x=to)

    def tokens_start():
        token_half(0, x, 0, right).start()
        token_half(1, x, 1, left).start()
        token_half(2, x, 1, right).start()
        token_half(2, x, 0, left).start()

    def tokens_forward():
        token_half(0, left, 0, right).wait_recv()
        token_half(3, left, 0, right).start()
        token_half(1, right, 1, left).wait_recv()
        token_half(3, right, 1, left).start()

    def tokens_near():
        taken(tok_rs.at[2], tokbuf.at[0, 0])

    def tokens_far():
        taken(tok_rs.at[3], tokbuf.at[0, 0])

    def to_all_x(ref_of, ss, rs):
        for k in (2, 1, 3):
            rc(ref_of(x), ref_of(x), ss, rs, x=at(x, k, nx)).start()

    def to_partner(owner, core):
        return rc(
            tokbuf.at[owner, core], tokbuf.at[owner, core], d2d_ss, d2d_rs, c=1 - c
        )

    def spikes(k, owner):
        return rc(spbuf.at[owner], spbuf.at[owner], sp_ss, sp_rs, x=at(x, k, nx))

    p1_send(0)
    pltpu.make_async_copy(tok_hbm, tok_ref, in_sems.at[0]).wait()
    small[0].wait()
    own = tok_ref[0].astype(F32)
    square = jnp.mean(own * own, axis=-1, keepdims=True)
    tokbuf[x, c] = (own * lax.rsqrt(square + EPS) * gin_ref[...]).astype(BF16)
    small[1].wait()
    spbuf[x] = spike_ref[0]
    fetched(2)
    tokens_start()
    to_partner(x, c).start()
    for k in range(1, nx):
        spikes(k, x).start()
    p1_send(1)

    pltpu.make_async_copy(wo_ref, wo_ref, in_sems.at[5]).wait()
    for copy in small[4:]:
        copy.wait()
    wobuf[...] = wo_ref[...].astype(F32)
    mine = pl.ds(pl.multiple_of(x * wo_cols, wo_cols), wo_cols)
    block = jnp.concatenate([wobuf[0, mine, :], wobuf[1, mine, :]], axis=0).astype(BF16)
    for p in range(2):
        wbuf[1, z, y, p] = block[:, p * WCOLS : (p + 1) * WCOLS]

    p1_wait(0)
    p2_own(0)
    tokens_forward()
    tokens_near()
    to_partner(left, c).start()
    to_partner(right, c).start()
    p2_relay(0)
    p1_wait(1)
    p2_own(1)
    p1_send(2)
    tokens_far()
    to_partner(across, c).start()
    taken(d2d_rs, tokbuf.at[:, 0])
    taken(sp_rs, spbuf.at[0 : nx - 1])
    p2_wait(0)

    rows = nx * TOK

    def project(weights):
        return nn(tokbuf[...].reshape(rows, width), weights).astype(BF16)

    projected = project(wbuf[0].reshape(width, WCOLS))
    fbuf[...] = projected[:, :HEAD]
    vbuf[...] = projected[:, HEAD:]

    ti = lax.broadcasted_iota(jnp.int32, (TOK, TOK), 0)
    si = lax.broadcasted_iota(jnp.int32, (TOK, TOK), 1)
    same = (ti // BLOCK) == (si // BLOCK)
    causal = jnp.logical_and(same, ti >= si)
    lower = causal.astype(F32)
    lower_b = lower.astype(BF16)
    ones_b = jnp.ones((TOK, HEAD), BF16)
    second = lax.broadcasted_iota(jnp.int32, (TOK, HEAD), 0) >= BLOCK
    lb_gate = 1.0 / (1.0 + jnp.exp(lb_ref[pl.ds(x, 1), :]))
    keys = lb_gate * (1.0 / (1.0 + jnp.exp(fbuf[...].astype(F32))))
    logs = three_parts(jnp.log(1.0 - keys))
    inners = []
    for s in range(nx):
        span = slice(s * TOK, (s + 1) * TOK)
        spread = three_parts(lower * spbuf[s, pl.ds(x, 1), :])
        inners.append(
            nn(
                jnp.concatenate([lower_b, lower_b, lower_b, *spread], axis=1),
                jnp.concatenate([*(part[span] for part in logs), ones_b, ones_b, ones_b], axis=0),
            )
        )
    decays, tails = [], []
    for s in range(nx):
        span = slice(s * TOK, (s + 1) * TOK)
        inner = inners[s]
        first_end = inner[BLOCK - 1 : BLOCK, :]
        total = first_end + inner[TOK - 1 : TOK, :]
        full = inner + jnp.where(second, first_end, 0.0)
        inner_buf[span, :] = inner
        cfull[span, :] = full
        tails.append((keys[span] * jnp.exp(total - full)).astype(BF16))
        decays.append(jnp.exp(total))
    for s in range(nx):
        state = tn(vbuf[s * TOK : (s + 1) * TOK, :], tails[s]).astype(BF16)
        for j in range(ny):
            c1_send[j, s * piece : (s + 1) * piece, :] = state[j * piece : (j + 1) * piece, :]

    def decay_rows(values):
        out = []
        for value in values:
            high = value.astype(BF16).astype(F32)
            out += [high, value - high]
        out.append(jnp.zeros((16 - len(out), HEAD), F32))
        return jnp.concatenate(out, axis=0).astype(BF16)

    extra = decay_rows(decays)
    for j in range(ny):
        c1_send[j, packed : packed + 16, :] = extra
    c1_recv[y] = c1_send[y]

    def c1(k, slot):
        to = at(y, k, ny)
        return rc(c1_send.at[to], c1_recv.at[slot], c1_ss, c1_rs, y=to)

    for k in far_first(ny):
        c1(k, y).start()

    p2_relay(1)

    taken(c1_rs, c1_send.at[0 : ny - 1])

    def read_decay(block, s):
        at_row = packed + 2 * s
        return block[at_row : at_row + 1, :] + block[at_row + 1 : at_row + 2, :]

    run = [jnp.zeros((piece, HEAD), F32) for _ in range(nx)]
    fade = [jnp.ones((1, HEAD), F32) for _ in range(nx)]
    for j in range(ny):
        block = c1_recv[j].astype(F32)
        for s in range(nx):
            pex[j, s * piece : (s + 1) * piece, :] = run[s]
            dex[j, s : s + 1, :] = fade[s]
            decay = read_decay(block, s)
            run[s] = decay * run[s] + block[s * piece : (s + 1) * piece, :]
            fade[s] = fade[s] * decay
    c2_send[0:packed, :] = jnp.concatenate(run, axis=0).astype(BF16)
    c2_send[packed : packed + 16, :] = decay_rows(fade)

    def c2(k, slot, to):
        return rc(c2_send, c2_recv.at[slot], c2_ss.at[k - 1], c2_rs.at[k - 1], z=to)

    if nz > 1:

        def send_later(k, _):
            c2(k, z, z + k).start()
            return _

        lax.fori_loop(1, nz - z, send_later, 0)

    p1_wait(2)
    p2_own(2)
    p2_wait(1, (1,))
    pbuf[...] = project(wqp[1].reshape(width, HEAD)).reshape(nx, TOK, HEAD)

    last = nz * ny - 1
    halo_src = pbuf.at[:, TOK - HALO : TOK]

    def halo_copy(**device):
        return rc(halo_src, halo, halo_ss, halo_rs, **device)

    if ny > 1:

        @pl.when(y < ny - 1)
        def _():
            halo_copy(y=y + 1).start()

    if nz > 1:

        @pl.when(jnp.logical_and(y == ny - 1, z < nz - 1))
        def _():
            halo_copy(z=z + 1, y=0).start()

    @pl.when(sp == 0)
    def _():
        halo[...] = jnp.zeros_like(halo)

    def add_row(zz, carry):
        if nz > 1:
            rc(
                c2_send, c2_recv.at[zz], c2_ss.at[z - zz - 1], c2_rs.at[z - zz - 1], z=zz
            ).wait_recv()
        block = c2_recv[zz].astype(F32)
        out = []
        for s in range(nx):
            out.append(
                read_decay(block, s) * carry[s] + block[s * piece : (s + 1) * piece, :]
            )
        return tuple(out)

    earlier = tuple(jnp.zeros((piece, HEAD), F32) for _ in range(nx))
    if nz > 1:
        earlier = lax.fori_loop(0, z, add_row, earlier)
    for j in range(ny):
        for s in range(nx):
            span = slice(s * piece, (s + 1) * piece)
            c3_send[j, span, :] = (dex[j, s : s + 1, :] * earlier[s] + pex[j, span, :]).astype(BF16)
    c3_recv[y] = c3_send[y]

    def c3(k, slot):
        to = at(y, k, ny)
        return rc(c3_send.at[to], c3_recv.at[slot], c3_ss, c3_rs, y=to)

    for k in far_first(ny):
        c3(k, y).start()

    if ny > 1:

        @pl.when(y > 0)
        def _():
            halo_copy(y=y - 1).wait_recv()

    if nz > 1:

        @pl.when(jnp.logical_and(y == 0, z > 0))
        def _():
            halo_copy(z=z - 1, y=ny - 1).wait_recv()

    group = (c * half_pool + x * HEAD) // WCOLS
    window = jnp.where(group == 0, 2, jnp.where(group == 1, 4, jnp.where(group == 2, 8, 16)))
    band = jnp.logical_and(ti >= si, ti - si < window).astype(BF16)
    hi = lax.broadcasted_iota(jnp.int32, (TOK, HALO), 0)
    hj = lax.broadcasted_iota(jnp.int32, (TOK, HALO), 1)
    band_before = (hi + HALO - hj < window).astype(BF16)
    place = sp * TOK + lax.broadcasted_iota(jnp.int32, (TOK, HEAD), 0) + 1
    count = jnp.minimum(place, window).astype(F32)
    for s in range(nx):
        sums = nn(band, pbuf[s]) + nn(band_before, halo[s])
        xpool[x, s * TOK : (s + 1) * TOK, :] = (sums / count - pbuf[s].astype(F32)).astype(BF16)

    to_all_x(lambda owner: xpool.at[owner], xp_ss, xp_rs)

    p2_wait(1, (0,))
    qbuf[...] = project(wqp[0].reshape(width, HEAD))

    for s in range(nx):
        span = slice(s * TOK, (s + 1) * TOK)
        query = qbuf[span, :].astype(F32)
        reader = query * (1.0 / (1.0 + jnp.exp(-query)))
        key = lb_gate * (1.0 / (1.0 + jnp.exp(fbuf[span, :].astype(F32))))
        inner = inner_buf[span, :]
        scaled = (reader * jnp.exp(inner)).astype(BF16)
        near = (key * jnp.exp(-inner)).astype(BF16)
        tail = (
            key[:BLOCK] * jnp.exp(inner[BLOCK - 1 : BLOCK, :] - inner[:BLOCK])
        ).astype(BF16)
        scores = nt(scaled, jnp.concatenate([near, tail], axis=0))
        cross = jnp.concatenate([scores[:, TOK:], scores[:, TOK:]], axis=1)
        before = jnp.logical_and(ti >= BLOCK, si < BLOCK)
        chosen = jnp.where(causal, scores[:, :TOK], jnp.where(before, cross, 0.0))
        within[span, :] = nn(chosen.astype(BF16), vbuf[span, :])
        cfull[span, :] = reader * jnp.exp(cfull[span, :])
    p2_relay(2)
    taken(c3_rs, c3_send.at[0 : ny - 1])
    gain = hg_ref[pl.ds(x, 1), :]

    def finish(s):
        span = slice(s * TOK, (s + 1) * TOK)
        prior = c3_recv[:, s * piece : (s + 1) * piece, :].reshape(HEAD, HEAD)
        read = within[span, :] + nt(cfull[span, :].astype(BF16), prior)
        square = jnp.mean(read * read, axis=-1, keepdims=True)
        normal = (read * lax.rsqrt(square + EPS) * gain).astype(BF16)
        xrec[x, s] = normal.reshape(2, HALF, HEAD)

    for s in range(nx):
        finish(s)
    to_all_x(lambda owner: xrec.at[owner], xr_ss, xr_rs)
    taken(xp_rs, xpool.at[0 : nx - 1])
    pieces = []
    for g in range(half_pool // WCOLS):
        cols = slice(g * WCOLS, (g + 1) * WCOLS)
        diff = jnp.concatenate([xpool[2 * g], xpool[2 * g + 1]], axis=1)
        pieces.append((nn(diff, maps_ref[g]) * scale_ref[:, cols]).astype(BF16))
    p2_wait(2)
    for p in range(2):
        both = wbuf[1, :, :, p].reshape(nz * ny, 2 * wo_cols, WCOLS).astype(F32)
        cols = slice(p * WCOLS, (p + 1) * WCOLS)
        wop[:, cols] = both[:, :wo_cols].reshape(nz * ny * wo_cols, WCOLS).astype(BF16)
        wor[:, cols] = both[:, wo_cols:].reshape(nz * ny * wo_cols, WCOLS).astype(BF16)
    pooled_out = nt(jnp.concatenate(pieces, axis=1), wop[...])
    pacc[...] = pooled_out.reshape(nx, 2, HALF, nz * ny * wo_cols)
    taken(xr_rs, xrec.at[0 : nx - 1])
    cols_out = nz * ny * wo_cols

    def to_half(s):
        return rc(parts.at[s, 1 - c], part_in.at[s], part_ss, part_rs.at[s], c=1 - c)

    def deliver(k, owner):
        to = at(x, k, nx)
        return rc(mixed.at[to], obuf.at[owner], o_ss, o_rs, x=to)

    order_x = (*far_first(nx), 0)
    def half_of(core):
        rec = jnp.concatenate([xrec[i, :, core].reshape(nx * HALF, HEAD) for i in range(nx)], axis=1)
        pooled = pacc[:, core].reshape(nx * HALF, cols_out)
        parts[:, core] = (pooled + nt(rec, wor[...])).astype(BF16).reshape(nx, HALF, cols_out)

    half_of(1 - c)
    for k in order_x:
        to_half(at(x, k, nx)).start()
    half_of(c)
    for k in order_x:
        s = at(x, k, nx)
        to_half(s).wait_recv()
        joint = (parts[s, c].astype(F32) + part_in[s].astype(F32)).astype(BF16)
        if k:
            mixed[s] = joint
            deliver(k, x).start()
        else:
            obuf[x] = joint
    taken(o_rs, mixed.at[0 : nx - 1])

    chunk = min(HEAD, cols_out)
    total_cols = chunk * nx
    src = lax.broadcasted_iota(jnp.int32, (total_cols, total_cols), 0)
    dst = lax.broadcasted_iota(jnp.int32, (total_cols, total_cols), 1)
    wanted = (
        lax.div(lax.rem(dst, 32), wo_cols) * chunk
        + lax.div(dst, 32) * wo_cols
        + lax.rem(dst, wo_cols)
    )
    order = (src == wanted).astype(BF16)
    for q in range(cols_out // chunk):
        cols = slice(q * chunk, (q + 1) * chunk)
        joined = jnp.concatenate([obuf[i, :, cols] for i in range(nx)], axis=1)
        out_ref[0, :, q * total_cols : (q + 1) * total_cols] = nn(joined, order).astype(BF16)

    for st in range(3):
        p1_done(st)
        p2_done(st)
    left_here(tok_ss, tokbuf.at[0:3, 0])
    left_here(d2d_ss, tokbuf.at[:, 0])
    left_here(sp_ss, spbuf.at[0 : nx - 1])
    left_here(c1_ss, c1_send.at[0 : ny - 1])
    left_here(c3_ss, c3_send.at[0 : ny - 1])
    left_here(xp_ss, xpool.at[0 : nx - 1])
    left_here(xr_ss, xrec.at[0 : nx - 1])
    left_here(o_ss, mixed.at[0 : nx - 1])
    left_here(part_ss, part_in)
    if nz > 1:

        def sent_later(k, _):
            c2(k, z, z + k).wait_send()
            return _

        lax.fori_loop(1, nz - z, sent_later, 0)
    @pl.when(sp < last)
    def _():
        halo_copy(c=1 - c).wait_send()


def body(sizes, *arrays):
    nz, ny, nx = sizes
    (tok, gin, wp, wq, wf, wv, maps, scale, lb, spike, hg, wpo, wro) = arrays
    width = tok.shape[2]
    rows = nx * TOK
    piece = HEAD // ny
    packed = nx * piece
    wo_cols = 32 // nx
    cols_out = nz * ny * wo_cols
    kdim = nx * HEAD
    ring_inputs = [
        pltpu.VMEM(tok.shape, BF16),
        pltpu.VMEM((1, width), F32),
        pltpu.VMEM(maps.shape, BF16),
        pltpu.VMEM((1, kdim), F32),
        pltpu.VMEM((nx, HEAD), F32),
        pltpu.VMEM((1, spike.shape[2], TOK), F32),
        pltpu.VMEM((nx, HEAD), F32),
        pltpu.VMEM((2, 32, kdim), BF16),
    ]
    scratch = [
        *ring_inputs,
        pltpu.VMEM((nx, 2, HALF, width), BF16),
        pltpu.VMEM((2, nz, ny, 2, WROWS, WCOLS), BF16),
        pltpu.VMEM((2, nz, ny, 2 * WROWS, HEAD), BF16),
        pltpu.VMEM((2, 32, kdim), F32),
        pltpu.VMEM((cols_out, kdim), BF16),
        pltpu.VMEM((cols_out, kdim), BF16),
        pltpu.VMEM((nx, spike.shape[2], TOK), F32),
        pltpu.VMEM((rows, HEAD), BF16),
        pltpu.VMEM((rows, HEAD), BF16),
        pltpu.VMEM((rows, HEAD), BF16),
        pltpu.VMEM((nx, TOK, HEAD), BF16),
        pltpu.VMEM((rows, HEAD), F32),
        pltpu.VMEM((rows, HEAD), F32),
        pltpu.VMEM((ny, packed + 16, HEAD), BF16),
        pltpu.VMEM((ny, packed + 16, HEAD), BF16),
        pltpu.VMEM((ny, packed, HEAD), F32),
        pltpu.VMEM((ny, 8, HEAD), F32),
        pltpu.VMEM((packed + 16, HEAD), BF16),
        pltpu.VMEM((nz, packed + 16, HEAD), BF16),
        pltpu.VMEM((ny, packed, HEAD), BF16),
        pltpu.VMEM((ny, packed, HEAD), BF16),
        pltpu.VMEM((nx, HALO, HEAD), BF16),
        pltpu.VMEM((rows, HEAD), F32),
        pltpu.VMEM((nx, rows, HEAD), BF16),
        pltpu.VMEM((nx, nx, 2, HALF, HEAD), BF16),
        pltpu.VMEM((nx, 2, HALF, cols_out), F32),
        pltpu.VMEM((nx, 2, HALF, cols_out), BF16),
        pltpu.VMEM((nx, HALF, cols_out), BF16),
        pltpu.VMEM((nx, HALF, cols_out), BF16),
        pltpu.VMEM((nx, HALF, cols_out), BF16),
        *[pltpu.SemaphoreType.DMA((3,))] * 2,
        pltpu.SemaphoreType.DMA((3,)),
        pltpu.SemaphoreType.DMA((3, PARTS)),
        pltpu.SemaphoreType.DMA((3, 2)),
        pltpu.SemaphoreType.DMA,
        pltpu.SemaphoreType.DMA((4,)),
        *[pltpu.SemaphoreType.DMA] * 2,
        *[pltpu.SemaphoreType.DMA] * 2,
        *[pltpu.SemaphoreType.DMA] * 2,
        *[pltpu.SemaphoreType.DMA((max(nz - 1, 1),))] * 2,
        *[pltpu.SemaphoreType.DMA] * 2,
        *[pltpu.SemaphoreType.DMA] * 2,
        *[pltpu.SemaphoreType.DMA] * 2,
        *[pltpu.SemaphoreType.DMA] * 2,
        pltpu.SemaphoreType.DMA,
        pltpu.SemaphoreType.DMA((nx,)),
        *[pltpu.SemaphoreType.DMA] * 2,
        pltpu.SemaphoreType.DMA((10,)),
    ]
    return pl.pallas_call(
        functools.partial(kernel, sizes),
        out_shape=jax.ShapeDtypeStruct(tok.shape, BF16),
        in_specs=[pl.BlockSpec(memory_space=pltpu.HBM)] * 13,
        out_specs=pl.BlockSpec(memory_space=pltpu.VMEM),
        scratch_shapes=scratch,
        compiler_params=pltpu.CompilerParams(
            collective_id=0, has_side_effects=True, vmem_limit_bytes=40 * 1024 * 1024
        ),
        name="layer",
    )(*map(pinned, (
        tok,
        gin.reshape(1, width),
        wp,
        wq,
        wf,
        wv,
        maps,
        scale.reshape(1, kdim),
        lb.reshape(nx, HEAD),
        jnp.swapaxes(spike, 1, 2),
        hg.reshape(nx, HEAD),
        wpo.T,
        wro.T,
    )))


def pinned(array):
    return pltpu.with_memory_space_constraint(array, pltpu.HBM)


def layout(devices, sizes):
    nz, ny, nx = sizes
    torus = Mesh(devices.reshape(nz, ny, nx, 2), ("z", "y", "x", "c"))
    sp = ("z", "y")
    return jax.shard_map(
        functools.partial(body, sizes),
        mesh=torus,
        in_specs=(
            P("x", ("z", "y", "c"), None),
            P(),
            P(sp, "c"),
            P(sp, "c"),
            P(sp, "c"),
            P(sp, "c"),
            P("c", None, None),
            P("c"),
            P("c"),
            P("x", sp, "c"),
            P("c"),
            P("c", sp),
            P("c", sp),
        ),
        out_specs=P("x", ("z", "y", "c"), None),
        check_vma=False,
    )


def solution(mesh):
    return layout(mesh.devices, (8, 8, mesh.shape["fs"]))
```

```python
import functools

import jax
import jax.numpy as jnp
from jax import lax
from jax.experimental import pallas as pl
from jax.experimental.pallas import tpu as pltpu
from jax.sharding import Mesh
from jax.sharding import PartitionSpec as P

MESH = pl.DeviceIdType.MESH
BLOCK = 64
HEAD = 128
TOK = 128
HALF = 64
WROWS = 16
WCOLS = 256
HALO = 16
PARTS = 2
EPS = 1e-06
F32 = jnp.float32
BF16 = jnp.bfloat16


def three_parts(value):
    high = value.astype(BF16)
    rest = value - high.astype(F32)
    mid = rest.astype(BF16)
    low = (rest - mid.astype(F32)).astype(BF16)
    return high, mid, low


def nt(a, b):
    return lax.dot_general(a, b, (((1,), (1,)), ((), ())), preferred_element_type=F32)


def tn(a, b):
    return lax.dot_general(a, b, (((0,), (0,)), ((), ())), preferred_element_type=F32)


def nn(a, b):
    return jnp.dot(a, b, preferred_element_type=F32)


def kernel(
    sizes,
    tok_hbm,
    gin_hbm,
    wp_hbm,
    wq_hbm,
    wf_hbm,
    wv_hbm,
    maps_hbm,
    scale_hbm,
    lb_hbm,
    spike_hbm,
    hg_hbm,
    wpo_hbm,
    wro_hbm,
    out_ref,
    tok_ref,
    gin_ref,
    maps_ref,
    scale_ref,
    lb_ref,
    spike_ref,
    hg_ref,
    wo_ref,
    tokbuf,
    wbuf,
    wqp,
    wobuf,
    wop,
    wor,
    spbuf,
    fbuf,
    vbuf,
    qbuf,
    pbuf,
    cfull,
    inner_buf,
    c1_send,
    c1_recv,
    pex,
    dex,
    c2_send,
    c2_recv,
    c3_send,
    c3_recv,
    halo,
    within,
    xpool,
    xrec,
    pacc,
    parts,
    part_in,
    mixed,
    obuf,
    order,
    p1_ss,
    p1_rs,
    p2_ss,
    p2_near,
    p2_rest,
    tok_ss,
    tok_rs,
    d2d_ss,
    d2d_rs,
    sp_ss,
    sp_rs,
    c1_ss,
    c1_rs,
    c2_ss,
    c2_rs,
    c3_ss,
    c3_rs,
    halo_ss,
    halo_rs,
    xp_ss,
    xp_rs,
    xr_ss,
    xr_rs,
    part_ss,
    part_rs,
    o_ss,
    o_rs,
    in_sems,
):
    nz, ny, nx = sizes
    z, y, x, c = (lax.axis_index(name) for name in ("z", "y", "x", "c"))
    sp = z * ny + y
    width = tok_hbm.shape[2]
    wo_cols = 32 // nx
    piece = HEAD // ny
    packed = nx * piece
    half_pool = nx * HEAD

    def rc(src, dst, ss, rs, **device):
        return pltpu.make_async_remote_copy(
            src_ref=src, dst_ref=dst, send_sem=ss, recv_sem=rs, device_id=device, device_id_type=MESH
        )

    def taken(sem, ref):
        rc(ref, ref, sp_ss, sem, c=1 - c).wait_recv()

    def left_here(sem, ref):
        rc(ref, ref, sem, sp_rs, c=1 - c).wait_send()

    def far_first(count):
        return sorted(range(1, count), key=lambda k: -min(k, count - k))

    def at(base, step, count):
        return lax.rem(base + step + count, count)

    pltpu.make_async_copy(tok_hbm, tok_ref, in_sems.at[0]).start()
    lanes = pl.ds(pl.multiple_of(x * HEAD, HEAD), HEAD)
    slices = []
    for n, ref in enumerate((wf_hbm, wv_hbm)):
        for p in range(2):
            slices.append(
                pltpu.make_async_copy(
                    ref.at[p * WROWS : (p + 1) * WROWS, lanes],
                    wbuf.at[0, z, y, p, :, pl.ds(n * HEAD, HEAD)],
                    in_sems.at[1],
                )
            )
    for n, ref in enumerate((wq_hbm, wp_hbm)):
        slices.append(
            pltpu.make_async_copy(ref.at[:, lanes], wqp.at[n, z, y], in_sems.at[2])
        )
    def fetched(n):
        pltpu.make_async_copy(wbuf.at[0, z, y], wbuf.at[0, z, y], in_sems.at[n]).wait()

    small = [
        pltpu.make_async_copy(src, dst, in_sems.at[3 + min(n, 2) if n < 4 else n + 2])
        for n, (src, dst) in enumerate(
            (
                (gin_hbm, gin_ref),
                (spike_hbm, spike_ref),
                (wpo_hbm, wo_ref.at[0]),
                (wro_hbm, wo_ref.at[1]),
                (lb_hbm, lb_ref),
                (hg_hbm, hg_ref),
                (scale_hbm, scale_ref),
                (maps_hbm, maps_ref),
            )
        )
    ]
    for copy in slices[:4] + small[:2] + slices[4:] + small[2:]:
        copy.start()

    barrier = pltpu.get_barrier_semaphore()

    def greet(**device):
        pl.semaphore_signal(barrier, inc=1, device_id=device, device_id_type=MESH)

    for k in range(1, ny):
        greet(y=at(y, k, ny))
    for k in range(1, nz):
        greet(z=at(z, k, nz))
    for k in range(1, nx):
        greet(x=at(x, k, nx))
    greet(c=1 - c)
    if nz > 1 and ny > 1:
        down = jnp.logical_and(y == ny - 1, z < nz - 1)
        up = jnp.logical_and(y == 0, z > 0)

        @pl.when(down)
        def _():
            greet(z=z + 1, y=0)

        @pl.when(up)
        def _():
            greet(z=z - 1, y=ny - 1)

    greeted = (ny - 1) + (nz - 1) + (nx - 1) + 1
    if nz > 1 and ny > 1:
        at_end = (y // (ny - 1)) * (1 - z // (nz - 1))
        at_start = ((ny - 1 - y) // (ny - 1)) * (1 - (nz - 1 - z) // (nz - 1))
        greeted = greeted + at_end + at_start
    fetched(1)
    pl.semaphore_wait(barrier, greeted)

    def wslot(st, path, zz, yy):
        return wqp.at[path, zz, yy] if st == 1 else wbuf.at[st // 2, zz, yy, path]

    def p1(st, k, path):
        if path == 0:
            return lambda zz, zt: rc(
                wslot(st, 0, zz, y),
                wslot(st, 0, zz, y),
                p1_ss.at[st],
                p1_rs.at[st],
                z=zt,
            )
        return lambda yy, yt: rc(
            wslot(st, 1, z, yy),
            wslot(st, 1, z, yy),
            p1_ss.at[st],
            p1_rs.at[st],
            y=yt,
        )

    def p1_send(st):
        for k in far_first(max(nz, ny)):
            if k < nz:
                p1(st, k, 0)(z, at(z, k, nz)).start()
            if k < ny:
                p1(st, k, 1)(y, at(y, k, ny)).start()

    def p1_wait(st):
        taken(p1_rs.at[st], wbuf.at[0, 0, 0 : ny - 1])

    def p1_done(st):
        left_here(p1_ss.at[st], wbuf.at[0, 0, 0 : ny - 1])

    paths = ((0, ny, nz), (1, nz, ny))

    def p2(st, path, way, source, distance, part):
        sign = 1 if way == 0 else -1
        if path == 0:
            size = nz // PARTS
            block = wslot(st, 0, pl.ds(part * size, size), at(y, -sign * source, ny))
            device = {"y": at(y, sign * max(distance - source, 1), ny)}
        else:
            size = ny // PARTS
            block = wslot(st, 1, at(z, -sign * source, nz), pl.ds(part * size, size))
            device = {"z": at(z, sign * max(distance - source, 1), nz)}
        arrives = p2_near.at[st, part] if distance == 2 else p2_rest.at[st, path]
        return rc(block, block, p2_ss.at[st], arrives, **device)

    def far_way(part):
        return 0 if part < PARTS // 2 else 1

    def each(part):
        return [(path, way, part) for path in range(2) for way in range(2)]

    def p2_own(st):
        for distance in (2, 1):
            for part in range(PARTS):
                for path, way, _ in each(part):
                    p2(st, path, way, 0, distance, part).start()

    def p2_relay(st):
        for part in range(PARTS):
            taken(p2_near.at[st, part], wbuf.at[0, 0, 0 : 2 * ny // PARTS])
            for path, way, _ in each(part):
                if way == far_way(part):
                    p2(st, path, way, 2, 4, part).start()
                p2(st, path, way, 2, 3, part).start()

    def p2_wait(st, only=(0, 1)):
        for path in only:
            taken(p2_rest.at[st, path], wbuf.at[0, 0:5, 0 : ny // 2])

    def p2_done(st):
        left_here(p2_ss.at[st], wbuf.at[0, 0 : nz - 1])

    right, left, across = at(x, 1, nx), at(x, -1, nx), at(x, 2, nx)

    def token_half(kind, owner, half, to):
        ref = tokbuf.at[owner, c, pl.ds(half * (HALF // 2), HALF // 2)]
        return rc(ref, ref, tok_ss, tok_rs.at[kind], x=to)

    def tokens_start():
        token_half(0, x, 0, right).start()
        token_half(1, x, 1, left).start()
        token_half(2, x, 1, right).start()
        token_half(2, x, 0, left).start()

    def tokens_forward():
        token_half(0, left, 0, right).wait_recv()
        token_half(3, left, 0, right).start()
        token_half(1, right, 1, left).wait_recv()
        token_half(3, right, 1, left).start()

    def tokens_near():
        taken(tok_rs.at[2], tokbuf.at[0, 0])

    def tokens_far():
        taken(tok_rs.at[3], tokbuf.at[0, 0])

    def to_all_x(ref_of, ss, rs):
        for k in (2, 1, 3):
            rc(ref_of(x), ref_of(x), ss, rs, x=at(x, k, nx)).start()

    def to_partner(owner, core):
        return rc(
            tokbuf.at[owner, core], tokbuf.at[owner, core], d2d_ss, d2d_rs, c=1 - c
        )

    def spikes(k, owner):
        return rc(spbuf.at[owner], spbuf.at[owner], sp_ss, sp_rs, x=at(x, k, nx))

    p1_send(0)
    pltpu.make_async_copy(tok_hbm, tok_ref, in_sems.at[0]).wait()
    small[0].wait()
    own = tok_ref[0].astype(F32)
    square = jnp.mean(own * own, axis=-1, keepdims=True)
    tokbuf[x, c] = (own * lax.rsqrt(square + EPS) * gin_ref[...]).astype(BF16)
    small[1].wait()
    spbuf[x] = spike_ref[0]
    fetched(2)
    tokens_start()
    to_partner(x, c).start()
    for k in range(1, nx):
        spikes(k, x).start()
    p1_send(1)

    pltpu.make_async_copy(wo_ref, wo_ref, in_sems.at[5]).wait()
    for copy in small[4:]:
        copy.wait()
    wobuf[...] = wo_ref[...].astype(F32)
    mine = pl.ds(pl.multiple_of(x * wo_cols, wo_cols), wo_cols)
    block = jnp.concatenate([wobuf[0, mine, :], wobuf[1, mine, :]], axis=0).astype(BF16)
    for p in range(2):
        wbuf[1, z, y, p] = block[:, p * WCOLS : (p + 1) * WCOLS]

    p1_wait(0)
    p2_own(0)
    tokens_forward()
    tokens_near()
    to_partner(left, c).start()
    to_partner(right, c).start()
    p2_relay(0)
    p1_wait(1)
    p2_own(1)
    p1_send(2)
    tokens_far()
    to_partner(across, c).start()
    taken(d2d_rs, tokbuf.at[:, 0])
    taken(sp_rs, spbuf.at[0 : nx - 1])
    p2_wait(0)

    rows = nx * TOK

    def project(weights):
        return nn(tokbuf[...].reshape(rows, width), weights).astype(BF16)

    projected = project(wbuf[0].reshape(width, WCOLS))
    fbuf[...] = projected[:, :HEAD]
    vbuf[...] = projected[:, HEAD:]

    ti = lax.broadcasted_iota(jnp.int32, (TOK, TOK), 0)
    si = lax.broadcasted_iota(jnp.int32, (TOK, TOK), 1)
    same = (ti // BLOCK) == (si // BLOCK)
    causal = jnp.logical_and(same, ti >= si)
    lower = causal.astype(F32)
    lower_b = lower.astype(BF16)
    ones_b = jnp.ones((TOK, HEAD), BF16)
    second = lax.broadcasted_iota(jnp.int32, (TOK, HEAD), 0) >= BLOCK
    lb_gate = 1.0 / (1.0 + jnp.exp(lb_ref[pl.ds(x, 1), :]))
    keys = lb_gate * (1.0 / (1.0 + jnp.exp(fbuf[...].astype(F32))))
    logs = three_parts(jnp.log(1.0 - keys))
    inners = []
    for s in range(nx):
        span = slice(s * TOK, (s + 1) * TOK)
        spread = three_parts(lower * spbuf[s, pl.ds(x, 1), :])
        inners.append(
            nn(
                jnp.concatenate([lower_b, lower_b, lower_b, *spread], axis=1),
                jnp.concatenate([*(part[span] for part in logs), ones_b, ones_b, ones_b], axis=0),
            )
        )
    decays, tails = [], []
    for s in range(nx):
        span = slice(s * TOK, (s + 1) * TOK)
        inner = inners[s]
        first_end = inner[BLOCK - 1 : BLOCK, :]
        total = first_end + inner[TOK - 1 : TOK, :]
        full = inner + jnp.where(second, first_end, 0.0)
        inner_buf[span, :] = inner
        cfull[span, :] = full
        tails.append((keys[span] * jnp.exp(total - full)).astype(BF16))
        decays.append(jnp.exp(total))
    for s in range(nx):
        state = tn(vbuf[s * TOK : (s + 1) * TOK, :], tails[s]).astype(BF16)
        for j in range(ny):
            c1_send[j, s * piece : (s + 1) * piece, :] = state[j * piece : (j + 1) * piece, :]

    def decay_rows(values):
        out = []
        for value in values:
            high = value.astype(BF16).astype(F32)
            out += [high, value - high]
        out.append(jnp.zeros((16 - len(out), HEAD), F32))
        return jnp.concatenate(out, axis=0).astype(BF16)

    extra = decay_rows(decays)
    for j in range(ny):
        c1_send[j, packed : packed + 16, :] = extra
    c1_recv[y] = c1_send[y]

    def c1(k, slot):
        to = at(y, k, ny)
        return rc(c1_send.at[to], c1_recv.at[slot], c1_ss, c1_rs, y=to)

    for k in far_first(ny):
        c1(k, y).start()

    p2_relay(1)

    taken(c1_rs, c1_send.at[0 : ny - 1])

    def read_decay(block, s):
        at_row = packed + 2 * s
        return block[at_row : at_row + 1, :] + block[at_row + 1 : at_row + 2, :]

    run = [jnp.zeros((piece, HEAD), F32) for _ in range(nx)]
    fade = [jnp.ones((1, HEAD), F32) for _ in range(nx)]
    for j in range(ny):
        block = c1_recv[j].astype(F32)
        for s in range(nx):
            pex[j, s * piece : (s + 1) * piece, :] = run[s]
            dex[j, s : s + 1, :] = fade[s]
            decay = read_decay(block, s)
            run[s] = decay * run[s] + block[s * piece : (s + 1) * piece, :]
            fade[s] = fade[s] * decay
    c2_send[0:packed, :] = jnp.concatenate(run, axis=0).astype(BF16)
    c2_send[packed : packed + 16, :] = decay_rows(fade)

    def c2(k, slot, to):
        return rc(c2_send, c2_recv.at[slot], c2_ss.at[k - 1], c2_rs.at[k - 1], z=to)

    if nz > 1:

        def send_later(k, _):
            c2(k, z, z + k).start()
            return _

        lax.fori_loop(1, nz - z, send_later, 0)

    p1_wait(2)
    p2_own(2)
    p2_wait(1, (1,))
    pbuf[...] = project(wqp[1].reshape(width, HEAD)).reshape(nx, TOK, HEAD)

    last = nz * ny - 1
    halo_src = pbuf.at[:, TOK - HALO : TOK]

    def halo_copy(**device):
        return rc(halo_src, halo, halo_ss, halo_rs, **device)

    if ny > 1:

        @pl.when(y < ny - 1)
        def _():
            halo_copy(y=y + 1).start()

    if nz > 1:

        @pl.when(jnp.logical_and(y == ny - 1, z < nz - 1))
        def _():
            halo_copy(z=z + 1, y=0).start()

    @pl.when(sp == 0)
    def _():
        halo[...] = jnp.zeros_like(halo)

    group = (c * half_pool + x * HEAD) // WCOLS
    window = jnp.where(group == 0, 2, jnp.where(group == 1, 4, jnp.where(group == 2, 8, 16)))
    band = jnp.logical_and(ti >= si, ti - si < window).astype(BF16)
    hi = lax.broadcasted_iota(jnp.int32, (HALO, HALO), 0)
    hj = lax.broadcasted_iota(jnp.int32, (HALO, HALO), 1)
    band_before = (hi + HALO - hj < window).astype(BF16)
    place = sp * TOK + lax.broadcasted_iota(jnp.int32, (TOK, HEAD), 0) + 1
    count = jnp.minimum(place, window).astype(F32)

    def pooled(sums, s, span):
        return (sums / count[span] - pbuf[s, span, :].astype(F32)).astype(BF16)

    for s in range(nx):
        sums = nn(band, pbuf[s])
        xpool[x, s, HALO:, :] = pooled(sums[HALO:], s, slice(HALO, TOK))
    to_all_x(lambda owner: xpool.at[owner, :, HALO:TOK], xp_ss, xp_rs)

    def add_row(zz, carry):
        if nz > 1:
            rc(
                c2_send, c2_recv.at[zz], c2_ss.at[z - zz - 1], c2_rs.at[z - zz - 1], z=zz
            ).wait_recv()
        block = c2_recv[zz].astype(F32)
        out = []
        for s in range(nx):
            out.append(
                read_decay(block, s) * carry[s] + block[s * piece : (s + 1) * piece, :]
            )
        return tuple(out)

    earlier = tuple(jnp.zeros((piece, HEAD), F32) for _ in range(nx))
    if nz > 1:
        earlier = lax.fori_loop(0, z, add_row, earlier)
    for j in range(ny):
        for s in range(nx):
            span = slice(s * piece, (s + 1) * piece)
            c3_send[j, span, :] = (dex[j, s : s + 1, :] * earlier[s] + pex[j, span, :]).astype(BF16)
    c3_recv[y] = c3_send[y]

    def c3(k, slot):
        to = at(y, k, ny)
        return rc(c3_send.at[to], c3_recv.at[slot], c3_ss, c3_rs, y=to)

    for k in far_first(ny):
        c3(k, y).start()

    if ny > 1:

        @pl.when(y > 0)
        def _():
            halo_copy(y=y - 1).wait_recv()

    if nz > 1:

        @pl.when(jnp.logical_and(y == 0, z > 0))
        def _():
            halo_copy(z=z - 1, y=ny - 1).wait_recv()

    for s in range(nx):
        sums = nn(band[:HALO], pbuf[s]) + nn(band_before, halo[s])
        xpool[x, s, :HALO, :] = pooled(sums, s, slice(0, HALO))
    to_all_x(lambda owner: xpool.at[owner, :, 0:HALO], xp_ss, xp_rs)

    p2_wait(1, (0,))
    qbuf[...] = project(wqp[0].reshape(width, HEAD))

    for s in range(nx):
        span = slice(s * TOK, (s + 1) * TOK)
        query = qbuf[span, :].astype(F32)
        reader = query * (1.0 / (1.0 + jnp.exp(-query)))
        key = lb_gate * (1.0 / (1.0 + jnp.exp(fbuf[span, :].astype(F32))))
        inner = inner_buf[span, :]
        scaled = (reader * jnp.exp(inner)).astype(BF16)
        near = (key * jnp.exp(-inner)).astype(BF16)
        tail = (
            key[:BLOCK] * jnp.exp(inner[BLOCK - 1 : BLOCK, :] - inner[:BLOCK])
        ).astype(BF16)
        scores = nt(scaled, jnp.concatenate([near, tail], axis=0))
        cross = jnp.concatenate([scores[:, TOK:], scores[:, TOK:]], axis=1)
        before = jnp.logical_and(ti >= BLOCK, si < BLOCK)
        chosen = jnp.where(causal, scores[:, :TOK], jnp.where(before, cross, 0.0))
        within[span, :] = nn(chosen.astype(BF16), vbuf[span, :])
        cfull[span, :] = reader * jnp.exp(cfull[span, :])
    p2_relay(2)
    chunk = min(HEAD, (nz * ny * wo_cols))
    total_cols = chunk * nx
    src = lax.broadcasted_iota(jnp.int32, (total_cols, total_cols), 0)
    dst = lax.broadcasted_iota(jnp.int32, (total_cols, total_cols), 1)
    wanted = (
        lax.div(lax.rem(dst, 32), wo_cols) * chunk
        + lax.div(dst, 32) * wo_cols
        + lax.rem(dst, wo_cols)
    )
    order[...] = (src == wanted).astype(BF16)
    taken(c3_rs, c3_send.at[0 : ny - 1])
    gain = hg_ref[pl.ds(x, 1), :]

    def finish(s):
        span = slice(s * TOK, (s + 1) * TOK)
        prior = c3_recv[:, s * piece : (s + 1) * piece, :].reshape(HEAD, HEAD)
        read = within[span, :] + nt(cfull[span, :].astype(BF16), prior)
        square = jnp.mean(read * read, axis=-1, keepdims=True)
        normal = (read * lax.rsqrt(square + EPS) * gain).astype(BF16)
        xrec[x, s] = normal.reshape(2, HALF, HEAD)

    for s in range(nx):
        finish(s)
    to_all_x(lambda owner: xrec.at[owner], xr_ss, xr_rs)
    taken(xp_rs, xpool.at[0 : nx - 1])
    pieces = []
    for g in range(half_pool // WCOLS):
        cols = slice(g * WCOLS, (g + 1) * WCOLS)
        diff = jnp.concatenate(
            [xpool[2 * g + n].reshape(rows, HEAD) for n in range(2)], axis=1
        )
        pieces.append((nn(diff, maps_ref[g]) * scale_ref[:, cols]).astype(BF16))
    p2_wait(2)
    for p in range(2):
        both = wbuf[1, :, :, p].reshape(nz * ny, 2 * wo_cols, WCOLS).astype(F32)
        cols = slice(p * WCOLS, (p + 1) * WCOLS)
        wop[:, cols] = both[:, :wo_cols].reshape(nz * ny * wo_cols, WCOLS).astype(BF16)
        wor[:, cols] = both[:, wo_cols:].reshape(nz * ny * wo_cols, WCOLS).astype(BF16)
    pooled_out = nt(jnp.concatenate(pieces, axis=1), wop[...])
    pacc[...] = pooled_out.reshape(nx, 2, HALF, nz * ny * wo_cols)
    taken(xr_rs, xrec.at[0 : nx - 1])
    cols_out = nz * ny * wo_cols

    def to_half(s):
        return rc(parts.at[s, 1 - c], part_in.at[s], part_ss, part_rs.at[s], c=1 - c)

    def deliver(k, owner):
        to = at(x, k, nx)
        return rc(mixed.at[to], obuf.at[owner], o_ss, o_rs, x=to)

    order_x = (*far_first(nx), 0)
    def half_of(core):
        rec = jnp.concatenate([xrec[i, :, core].reshape(nx * HALF, HEAD) for i in range(nx)], axis=1)
        pooled = pacc[:, core].reshape(nx * HALF, cols_out)
        parts[:, core] = (pooled + nt(rec, wor[...])).astype(BF16).reshape(nx, HALF, cols_out)

    half_of(1 - c)
    for k in order_x:
        to_half(at(x, k, nx)).start()
    half_of(c)
    for k in order_x:
        s = at(x, k, nx)
        to_half(s).wait_recv()
        joint = (parts[s, c].astype(F32) + part_in[s].astype(F32)).astype(BF16)
        if k:
            mixed[s] = joint
            deliver(k, x).start()
        else:
            obuf[x] = joint
    taken(o_rs, mixed.at[0 : nx - 1])

    joined = [
        jnp.concatenate([obuf[i, :, q * chunk : (q + 1) * chunk] for i in range(nx)], axis=1)
        for q in range(cols_out // chunk)
    ]
    ordered = nn(jnp.concatenate(joined, axis=0), order[...]).astype(BF16)
    for q in range(cols_out // chunk):
        out_ref[0, :, q * total_cols : (q + 1) * total_cols] = ordered[q * HALF : (q + 1) * HALF]

    for st in range(3):
        p1_done(st)
        p2_done(st)
    left_here(tok_ss, tokbuf.at[0:3, 0])
    left_here(d2d_ss, tokbuf.at[:, 0])
    left_here(sp_ss, spbuf.at[0 : nx - 1])
    left_here(c1_ss, c1_send.at[0 : ny - 1])
    left_here(c3_ss, c3_send.at[0 : ny - 1])
    left_here(xp_ss, xpool.at[0 : nx - 1])
    left_here(xr_ss, xrec.at[0 : nx - 1])
    left_here(o_ss, mixed.at[0 : nx - 1])
    left_here(part_ss, part_in)
    if nz > 1:

        def sent_later(k, _):
            c2(k, z, z + k).wait_send()
            return _

        lax.fori_loop(1, nz - z, sent_later, 0)
    @pl.when(sp < last)
    def _():
        halo_copy(c=1 - c).wait_send()


def body(sizes, *arrays):
    nz, ny, nx = sizes
    (tok, gin, wp, wq, wf, wv, maps, scale, lb, spike, hg, wpo, wro) = arrays
    width = tok.shape[2]
    rows = nx * TOK
    piece = HEAD // ny
    packed = nx * piece
    wo_cols = 32 // nx
    cols_out = nz * ny * wo_cols
    kdim = nx * HEAD
    ring_inputs = [
        pltpu.VMEM(tok.shape, BF16),
        pltpu.VMEM((1, width), F32),
        pltpu.VMEM(maps.shape, BF16),
        pltpu.VMEM((1, kdim), F32),
        pltpu.VMEM((nx, HEAD), F32),
        pltpu.VMEM((1, spike.shape[2], TOK), F32),
        pltpu.VMEM((nx, HEAD), F32),
        pltpu.VMEM((2, 32, kdim), BF16),
    ]
    scratch = [
        *ring_inputs,
        pltpu.VMEM((nx, 2, HALF, width), BF16),
        pltpu.VMEM((2, nz, ny, 2, WROWS, WCOLS), BF16),
        pltpu.VMEM((2, nz, ny, 2 * WROWS, HEAD), BF16),
        pltpu.VMEM((2, 32, kdim), F32),
        pltpu.VMEM((cols_out, kdim), BF16),
        pltpu.VMEM((cols_out, kdim), BF16),
        pltpu.VMEM((nx, spike.shape[2], TOK), F32),
        pltpu.VMEM((rows, HEAD), BF16),
        pltpu.VMEM((rows, HEAD), BF16),
        pltpu.VMEM((rows, HEAD), BF16),
        pltpu.VMEM((nx, TOK, HEAD), BF16),
        pltpu.VMEM((rows, HEAD), F32),
        pltpu.VMEM((rows, HEAD), F32),
        pltpu.VMEM((ny, packed + 16, HEAD), BF16),
        pltpu.VMEM((ny, packed + 16, HEAD), BF16),
        pltpu.VMEM((ny, packed, HEAD), F32),
        pltpu.VMEM((ny, 8, HEAD), F32),
        pltpu.VMEM((packed + 16, HEAD), BF16),
        pltpu.VMEM((nz, packed + 16, HEAD), BF16),
        pltpu.VMEM((ny, packed, HEAD), BF16),
        pltpu.VMEM((ny, packed, HEAD), BF16),
        pltpu.VMEM((nx, HALO, HEAD), BF16),
        pltpu.VMEM((rows, HEAD), F32),
        pltpu.VMEM((nx, nx, TOK, HEAD), BF16),
        pltpu.VMEM((nx, nx, 2, HALF, HEAD), BF16),
        pltpu.VMEM((nx, 2, HALF, cols_out), F32),
        pltpu.VMEM((nx, 2, HALF, cols_out), BF16),
        pltpu.VMEM((nx, HALF, cols_out), BF16),
        pltpu.VMEM((nx, HALF, cols_out), BF16),
        pltpu.VMEM((nx, HALF, cols_out), BF16),
        pltpu.VMEM((nx * min(HEAD, cols_out), nx * min(HEAD, cols_out)), BF16),
        *[pltpu.SemaphoreType.DMA((3,))] * 2,
        pltpu.SemaphoreType.DMA((3,)),
        pltpu.SemaphoreType.DMA((3, PARTS)),
        pltpu.SemaphoreType.DMA((3, 2)),
        pltpu.SemaphoreType.DMA,
        pltpu.SemaphoreType.DMA((4,)),
        *[pltpu.SemaphoreType.DMA] * 2,
        *[pltpu.SemaphoreType.DMA] * 2,
        *[pltpu.SemaphoreType.DMA] * 2,
        *[pltpu.SemaphoreType.DMA((max(nz - 1, 1),))] * 2,
        *[pltpu.SemaphoreType.DMA] * 2,
        *[pltpu.SemaphoreType.DMA] * 2,
        *[pltpu.SemaphoreType.DMA] * 2,
        *[pltpu.SemaphoreType.DMA] * 2,
        pltpu.SemaphoreType.DMA,
        pltpu.SemaphoreType.DMA((nx,)),
        *[pltpu.SemaphoreType.DMA] * 2,
        pltpu.SemaphoreType.DMA((10,)),
    ]
    return pl.pallas_call(
        functools.partial(kernel, sizes),
        out_shape=jax.ShapeDtypeStruct(tok.shape, BF16),
        in_specs=[pl.BlockSpec(memory_space=pltpu.HBM)] * 13,
        out_specs=pl.BlockSpec(memory_space=pltpu.VMEM),
        scratch_shapes=scratch,
        compiler_params=pltpu.CompilerParams(
            collective_id=0, has_side_effects=True, vmem_limit_bytes=40 * 1024 * 1024
        ),
        name="layer",
    )(*map(pinned, (
        tok,
        gin.reshape(1, width),
        wp,
        wq,
        wf,
        wv,
        maps,
        scale.reshape(1, kdim),
        lb.reshape(nx, HEAD),
        jnp.swapaxes(spike, 1, 2),
        hg.reshape(nx, HEAD),
        wpo.T,
        wro.T,
    )))


def pinned(array):
    return pltpu.with_memory_space_constraint(array, pltpu.HBM)


def layout(devices, sizes):
    nz, ny, nx = sizes
    torus = Mesh(devices.reshape(nz, ny, nx, 2), ("z", "y", "x", "c"))
    sp = ("z", "y")
    return jax.shard_map(
        functools.partial(body, sizes),
        mesh=torus,
        in_specs=(
            P("x", ("z", "y", "c"), None),
            P(),
            P(sp, "c"),
            P(sp, "c"),
            P(sp, "c"),
            P(sp, "c"),
            P("c", None, None),
            P("c"),
            P("c"),
            P("x", sp, "c"),
            P("c"),
            P("c", sp),
            P("c", sp),
        ),
        out_specs=P("x", ("z", "y", "c"), None),
        check_vma=False,
    )


def solution(mesh):
    return layout(mesh.devices, (8, 8, mesh.shape["fs"]))
```

```python
import functools

import jax
import jax.numpy as jnp
from jax import lax
from jax.experimental import pallas as pl
from jax.experimental.pallas import tpu as pltpu
from jax.sharding import Mesh
from jax.sharding import PartitionSpec as P

MESH = pl.DeviceIdType.MESH
BLOCK = 64
HEAD = 128
TOK = 128
HALF = 64
WROWS = 16
WCOLS = 256
HALO = 16
PARTS = 2
EPS = 1e-06
F32 = jnp.float32
BF16 = jnp.bfloat16


def three_parts(value):
    high = value.astype(BF16)
    rest = value - high.astype(F32)
    mid = rest.astype(BF16)
    low = (rest - mid.astype(F32)).astype(BF16)
    return high, mid, low


def nt(a, b):
    return lax.dot_general(a, b, (((1,), (1,)), ((), ())), preferred_element_type=F32)


def tn(a, b):
    return lax.dot_general(a, b, (((0,), (0,)), ((), ())), preferred_element_type=F32)


def nn(a, b):
    return jnp.dot(a, b, preferred_element_type=F32)


def kernel(
    sizes,
    tok_hbm,
    gin_hbm,
    wp_hbm,
    wq_hbm,
    wf_hbm,
    wv_hbm,
    maps_hbm,
    scale_hbm,
    lb_hbm,
    spike_hbm,
    hg_hbm,
    wpo_hbm,
    wro_hbm,
    out_ref,
    tok_ref,
    gin_ref,
    maps_ref,
    scale_ref,
    lb_ref,
    spike_ref,
    hg_ref,
    wo_ref,
    tokbuf,
    wbuf,
    wqp,
    wobuf,
    wop,
    wor,
    spbuf,
    fbuf,
    vbuf,
    qbuf,
    pbuf,
    cfull,
    inner_buf,
    c1_send,
    c1_recv,
    pex,
    dex,
    c2_send,
    c2_recv,
    c3_send,
    c3_recv,
    halo,
    within,
    xpool,
    xrec,
    pacc,
    parts,
    part_in,
    mixed,
    obuf,
    order,
    p1_ss,
    p1_rs,
    p2_ss,
    p2_near,
    p2_rest,
    tok_ss,
    tok_rs,
    d2d_ss,
    d2d_rs,
    sp_ss,
    sp_rs,
    c1_ss,
    c1_rs,
    c2_ss,
    c2_rs,
    c3_ss,
    c3_rs,
    halo_ss,
    halo_rs,
    xp_ss,
    xp_rs,
    xr_ss,
    xr_rs,
    part_ss,
    part_rs,
    o_ss,
    o_rs,
    in_sems,
):
    nz, ny, nx = sizes
    z, y, x, c = (lax.axis_index(name) for name in ("z", "y", "x", "c"))
    sp = z * ny + y
    width = tok_hbm.shape[2]
    wo_cols = 32 // nx
    piece = HEAD // ny
    packed = nx * piece
    half_pool = nx * HEAD

    def rc(src, dst, ss, rs, **device):
        return pltpu.make_async_remote_copy(
            src_ref=src, dst_ref=dst, send_sem=ss, recv_sem=rs, device_id=device, device_id_type=MESH
        )

    def taken(sem, ref):
        rc(ref, ref, sp_ss, sem, c=1 - c).wait_recv()

    def left_here(sem, ref):
        rc(ref, ref, sem, sp_rs, c=1 - c).wait_send()

    def far_first(count):
        return sorted(range(1, count), key=lambda k: -min(k, count - k))

    def at(base, step, count):
        return lax.rem(base + step + count, count)

    pltpu.make_async_copy(tok_hbm, tok_ref, in_sems.at[0]).start()
    lanes = pl.ds(pl.multiple_of(x * HEAD, HEAD), HEAD)
    slices = []
    for n, ref in enumerate((wf_hbm, wv_hbm)):
        for p in range(2):
            slices.append(
                pltpu.make_async_copy(
                    ref.at[p * WROWS : (p + 1) * WROWS, lanes],
                    wbuf.at[0, z, y, p, :, pl.ds(n * HEAD, HEAD)],
                    in_sems.at[1],
                )
            )
    for n, ref in enumerate((wq_hbm, wp_hbm)):
        slices.append(
            pltpu.make_async_copy(ref.at[:, lanes], wqp.at[n, z, y], in_sems.at[2])
        )
    def fetched(n):
        pltpu.make_async_copy(wbuf.at[0, z, y], wbuf.at[0, z, y], in_sems.at[n]).wait()

    small = [
        pltpu.make_async_copy(src, dst, in_sems.at[3 + min(n, 2) if n < 4 else n + 2])
        for n, (src, dst) in enumerate(
            (
                (gin_hbm, gin_ref),
                (spike_hbm, spike_ref),
                (wpo_hbm, wo_ref.at[0]),
                (wro_hbm, wo_ref.at[1]),
                (lb_hbm, lb_ref),
                (hg_hbm, hg_ref),
                (scale_hbm, scale_ref),
                (maps_hbm, maps_ref),
            )
        )
    ]
    for copy in slices[:4] + small[:2] + slices[4:] + small[2:]:
        copy.start()

    barrier = pltpu.get_barrier_semaphore()

    def greet(**device):
        pl.semaphore_signal(barrier, inc=1, device_id=device, device_id_type=MESH)

    for k in range(1, ny):
        greet(y=at(y, k, ny))
    for k in range(1, nz):
        greet(z=at(z, k, nz))
    for k in range(1, nx):
        greet(x=at(x, k, nx))
    greet(c=1 - c)
    if nz > 1 and ny > 1:
        down = jnp.logical_and(y == ny - 1, z < nz - 1)
        up = jnp.logical_and(y == 0, z > 0)

        @pl.when(down)
        def _():
            greet(z=z + 1, y=0)

        @pl.when(up)
        def _():
            greet(z=z - 1, y=ny - 1)

    greeted = (ny - 1) + (nz - 1) + (nx - 1) + 1
    if nz > 1 and ny > 1:
        at_end = (y // (ny - 1)) * (1 - z // (nz - 1))
        at_start = ((ny - 1 - y) // (ny - 1)) * (1 - (nz - 1 - z) // (nz - 1))
        greeted = greeted + at_end + at_start
    fetched(1)
    pl.semaphore_wait(barrier, greeted)

    def wslot(st, path, zz, yy):
        return wqp.at[path, zz, yy] if st == 1 else wbuf.at[st // 2, zz, yy, path]

    def p1(st, k, path):
        if path == 0:
            return lambda zz, zt: rc(
                wslot(st, 0, zz, y),
                wslot(st, 0, zz, y),
                p1_ss.at[st],
                p1_rs.at[st],
                z=zt,
            )
        return lambda yy, yt: rc(
            wslot(st, 1, z, yy),
            wslot(st, 1, z, yy),
            p1_ss.at[st],
            p1_rs.at[st],
            y=yt,
        )

    def p1_send(st):
        for k in far_first(max(nz, ny)):
            if k < nz:
                p1(st, k, 0)(z, at(z, k, nz)).start()
            if k < ny:
                p1(st, k, 1)(y, at(y, k, ny)).start()

    def p1_wait(st):
        taken(p1_rs.at[st], wbuf.at[0, 0, 0 : ny - 1])

    def p1_done(st):
        left_here(p1_ss.at[st], wbuf.at[0, 0, 0 : ny - 1])

    paths = ((0, ny, nz), (1, nz, ny))

    def p2(st, path, way, source, distance, part):
        sign = 1 if way == 0 else -1
        if path == 0:
            size = nz // PARTS
            block = wslot(st, 0, pl.ds(part * size, size), at(y, -sign * source, ny))
            device = {"y": at(y, sign * max(distance - source, 1), ny)}
        else:
            size = ny // PARTS
            block = wslot(st, 1, at(z, -sign * source, nz), pl.ds(part * size, size))
            device = {"z": at(z, sign * max(distance - source, 1), nz)}
        arrives = p2_near.at[st, part] if distance == 2 else p2_rest.at[st, path]
        return rc(block, block, p2_ss.at[st], arrives, **device)

    def far_way(part):
        return 0 if part < PARTS // 2 else 1

    def each(part):
        return [(path, way, part) for path in range(2) for way in range(2)]

    def p2_own(st):
        for distance in (2, 1):
            for part in range(PARTS):
                for path, way, _ in each(part):
                    p2(st, path, way, 0, distance, part).start()

    def p2_relay(st):
        for part in range(PARTS):
            taken(p2_near.at[st, part], wbuf.at[0, 0, 0 : 2 * ny // PARTS])
            for path, way, _ in each(part):
                if way == far_way(part):
                    p2(st, path, way, 2, 4, part).start()
                p2(st, path, way, 2, 3, part).start()

    def p2_wait(st, only=(0, 1)):
        for path in only:
            taken(p2_rest.at[st, path], wbuf.at[0, 0:5, 0 : ny // 2])

    def p2_done(st):
        left_here(p2_ss.at[st], wbuf.at[0, 0 : nz - 1])

    right, left, across = at(x, 1, nx), at(x, -1, nx), at(x, 2, nx)

    def token_half(kind, owner, half, to):
        ref = tokbuf.at[owner, c, pl.ds(half * (HALF // 2), HALF // 2)]
        return rc(ref, ref, tok_ss, tok_rs.at[kind], x=to)

    def tokens_start():
        token_half(0, x, 0, right).start()
        token_half(1, x, 1, left).start()
        token_half(2, x, 1, right).start()
        token_half(2, x, 0, left).start()

    def tokens_forward():
        token_half(0, left, 0, right).wait_recv()
        token_half(3, left, 0, right).start()
        token_half(1, right, 1, left).wait_recv()
        token_half(3, right, 1, left).start()

    def tokens_near():
        taken(tok_rs.at[2], tokbuf.at[0, 0])

    def tokens_far():
        taken(tok_rs.at[3], tokbuf.at[0, 0])

    def to_all_x(ref_of, ss, rs):
        for k in (2, 1, 3):
            rc(ref_of(x), ref_of(x), ss, rs, x=at(x, k, nx)).start()

    def to_partner(owner, core):
        return rc(
            tokbuf.at[owner, core], tokbuf.at[owner, core], d2d_ss, d2d_rs, c=1 - c
        )

    def spikes(k, owner):
        return rc(spbuf.at[owner], spbuf.at[owner], sp_ss, sp_rs, x=at(x, k, nx))

    p1_send(0)
    pltpu.make_async_copy(tok_hbm, tok_ref, in_sems.at[0]).wait()
    small[0].wait()
    own = tok_ref[0].astype(F32)
    square = jnp.mean(own * own, axis=-1, keepdims=True)
    tokbuf[x, c] = (own * lax.rsqrt(square + EPS) * gin_ref[...]).astype(BF16)
    small[1].wait()
    spbuf[x] = spike_ref[0]
    fetched(2)
    tokens_start()
    to_partner(x, c).start()
    for k in range(1, nx):
        spikes(k, x).start()
    p1_send(1)

    pltpu.make_async_copy(wo_ref, wo_ref, in_sems.at[5]).wait()
    for copy in small[4:]:
        copy.wait()
    wobuf[...] = wo_ref[...].astype(F32)
    mine = pl.ds(pl.multiple_of(x * wo_cols, wo_cols), wo_cols)
    block = jnp.concatenate([wobuf[0, mine, :], wobuf[1, mine, :]], axis=0).astype(BF16)
    for p in range(2):
        wbuf[1, z, y, p] = block[:, p * WCOLS : (p + 1) * WCOLS]

    p1_wait(0)
    p2_own(0)
    tokens_forward()
    tokens_near()
    to_partner(left, c).start()
    to_partner(right, c).start()
    p2_relay(0)
    p1_wait(1)
    p2_own(1)
    p1_send(2)
    tokens_far()
    to_partner(across, c).start()
    taken(d2d_rs, tokbuf.at[:, 0])
    taken(sp_rs, spbuf.at[0 : nx - 1])
    p2_wait(0)

    rows = nx * TOK

    def project(weights):
        return nn(tokbuf[...].reshape(rows, width), weights).astype(BF16)

    projected = project(wbuf[0].reshape(width, WCOLS))
    fbuf[...] = projected[:, :HEAD]
    vbuf[...] = projected[:, HEAD:]

    ti = lax.broadcasted_iota(jnp.int32, (TOK, TOK), 0)
    si = lax.broadcasted_iota(jnp.int32, (TOK, TOK), 1)
    same = (ti // BLOCK) == (si // BLOCK)
    causal = jnp.logical_and(same, ti >= si)
    lower = causal.astype(F32)
    lower_b = lower.astype(BF16)
    ones_b = jnp.ones((TOK, HEAD), BF16)
    second = lax.broadcasted_iota(jnp.int32, (TOK, HEAD), 0) >= BLOCK
    lb_gate = 1.0 / (1.0 + jnp.exp(lb_ref[pl.ds(x, 1), :]))
    keys = lb_gate * (1.0 / (1.0 + jnp.exp(fbuf[...].astype(F32))))
    logs = three_parts(jnp.log(1.0 - keys))
    inners = []
    for s in range(nx):
        span = slice(s * TOK, (s + 1) * TOK)
        spread = three_parts(lower * spbuf[s, pl.ds(x, 1), :])
        inners.append(
            nn(
                jnp.concatenate([lower_b, lower_b, lower_b, *spread], axis=1),
                jnp.concatenate([*(part[span] for part in logs), ones_b, ones_b, ones_b], axis=0),
            )
        )
    decays, tails = [], []
    for s in range(nx):
        span = slice(s * TOK, (s + 1) * TOK)
        inner = inners[s]
        first_end = inner[BLOCK - 1 : BLOCK, :]
        total = first_end + inner[TOK - 1 : TOK, :]
        full = inner + jnp.where(second, first_end, 0.0)
        inner_buf[span, :] = inner
        cfull[span, :] = full
        tails.append((keys[span] * jnp.exp(total - full)).astype(BF16))
        decays.append(jnp.exp(total))
    for s in range(nx):
        state = tn(vbuf[s * TOK : (s + 1) * TOK, :], tails[s]).astype(BF16)
        for j in range(ny):
            c1_send[j, s * piece : (s + 1) * piece, :] = state[j * piece : (j + 1) * piece, :]

    def decay_rows(values):
        out = []
        for value in values:
            high = value.astype(BF16).astype(F32)
            out += [high, value - high]
        out.append(jnp.zeros((16 - len(out), HEAD), F32))
        return jnp.concatenate(out, axis=0).astype(BF16)

    extra = decay_rows(decays)
    for j in range(ny):
        c1_send[j, packed : packed + 16, :] = extra
    c1_recv[y] = c1_send[y]

    def c1(k, slot):
        to = at(y, k, ny)
        return rc(c1_send.at[to], c1_recv.at[slot], c1_ss, c1_rs, y=to)

    for k in far_first(ny):
        c1(k, y).start()

    p2_relay(1)

    taken(c1_rs, c1_send.at[0 : ny - 1])

    def read_decay(block, s):
        at_row = packed + 2 * s
        return block[at_row : at_row + 1, :] + block[at_row + 1 : at_row + 2, :]

    run = [jnp.zeros((piece, HEAD), F32) for _ in range(nx)]
    fade = [jnp.ones((1, HEAD), F32) for _ in range(nx)]
    for j in range(ny):
        block = c1_recv[j].astype(F32)
        for s in range(nx):
            pex[j, s * piece : (s + 1) * piece, :] = run[s]
            dex[j, s : s + 1, :] = fade[s]
            decay = read_decay(block, s)
            run[s] = decay * run[s] + block[s * piece : (s + 1) * piece, :]
            fade[s] = fade[s] * decay
    c2_send[0:packed, :] = jnp.concatenate(run, axis=0).astype(BF16)
    c2_send[packed : packed + 16, :] = decay_rows(fade)

    def c2(k, slot, to):
        return rc(c2_send, c2_recv.at[slot], c2_ss.at[k - 1], c2_rs.at[k - 1], z=to)

    if nz > 1:

        def send_later(k, _):
            c2(k, z, z + k).start()
            return _

        lax.fori_loop(1, nz - z, send_later, 0)

    p1_wait(2)
    p2_own(2)
    p2_wait(1, (1,))
    pbuf[...] = project(wqp[1].reshape(width, HEAD)).reshape(nx, TOK, HEAD)

    last = nz * ny - 1
    halo_src = pbuf.at[:, TOK - HALO : TOK]

    def halo_copy(**device):
        return rc(halo_src, halo, halo_ss, halo_rs, **device)

    if ny > 1:

        @pl.when(y < ny - 1)
        def _():
            halo_copy(y=y + 1).start()

    if nz > 1:

        @pl.when(jnp.logical_and(y == ny - 1, z < nz - 1))
        def _():
            halo_copy(z=z + 1, y=0).start()

    @pl.when(sp == 0)
    def _():
        halo[...] = jnp.zeros_like(halo)

    group = (c * half_pool + x * HEAD) // WCOLS
    window = jnp.where(group == 0, 2, jnp.where(group == 1, 4, jnp.where(group == 2, 8, 16)))
    band = jnp.logical_and(ti >= si, ti - si < window).astype(BF16)
    hi = lax.broadcasted_iota(jnp.int32, (HALO, HALO), 0)
    hj = lax.broadcasted_iota(jnp.int32, (HALO, HALO), 1)
    band_before = (hi + HALO - hj < window).astype(BF16)
    place = sp * TOK + lax.broadcasted_iota(jnp.int32, (TOK, HEAD), 0) + 1
    count = jnp.minimum(place, window).astype(F32)

    def pooled(sums, s, span):
        return (sums / count[span] - pbuf[s, span, :].astype(F32)).astype(BF16)

    for s in range(nx):
        sums = nn(band, pbuf[s])
        xpool[x, s, HALO:, :] = pooled(sums[HALO:], s, slice(HALO, TOK))
    to_all_x(lambda owner: xpool.at[owner, :, HALO:TOK], xp_ss, xp_rs)

    def add_row(zz, carry):
        if nz > 1:
            rc(
                c2_send, c2_recv.at[zz], c2_ss.at[z - zz - 1], c2_rs.at[z - zz - 1], z=zz
            ).wait_recv()
        block = c2_recv[zz].astype(F32)
        out = []
        for s in range(nx):
            out.append(
                read_decay(block, s) * carry[s] + block[s * piece : (s + 1) * piece, :]
            )
        return tuple(out)

    earlier = tuple(jnp.zeros((piece, HEAD), F32) for _ in range(nx))
    if nz > 1:
        earlier = lax.fori_loop(0, z, add_row, earlier)
    for j in range(ny):
        for s in range(nx):
            span = slice(s * piece, (s + 1) * piece)
            c3_send[j, span, :] = (dex[j, s : s + 1, :] * earlier[s] + pex[j, span, :]).astype(BF16)
    c3_recv[y] = c3_send[y]

    def c3(k, slot):
        to = at(y, k, ny)
        return rc(c3_send.at[to], c3_recv.at[slot], c3_ss, c3_rs, y=to)

    for k in far_first(ny):
        c3(k, y).start()

    if ny > 1:

        @pl.when(y > 0)
        def _():
            halo_copy(y=y - 1).wait_recv()

    if nz > 1:

        @pl.when(jnp.logical_and(y == 0, z > 0))
        def _():
            halo_copy(z=z - 1, y=ny - 1).wait_recv()

    for s in range(nx):
        sums = nn(band[:HALO], pbuf[s]) + nn(band_before, halo[s])
        xpool[x, s, :HALO, :] = pooled(sums, s, slice(0, HALO))
    to_all_x(lambda owner: xpool.at[owner, :, 0:HALO], xp_ss, xp_rs)

    p2_wait(1, (0,))
    qbuf[...] = project(wqp[0].reshape(width, HEAD))

    for s in range(nx):
        span = slice(s * TOK, (s + 1) * TOK)
        query = qbuf[span, :].astype(F32)
        reader = query * (1.0 / (1.0 + jnp.exp(-query)))
        key = lb_gate * (1.0 / (1.0 + jnp.exp(fbuf[span, :].astype(F32))))
        inner = inner_buf[span, :]
        scaled = (reader * jnp.exp(inner)).astype(BF16)
        near = (key * jnp.exp(-inner)).astype(BF16)
        tail = (
            key[:BLOCK] * jnp.exp(inner[BLOCK - 1 : BLOCK, :] - inner[:BLOCK])
        ).astype(BF16)
        scores = nt(scaled, jnp.concatenate([near, tail], axis=0))
        cross = jnp.concatenate([scores[:, TOK:], scores[:, TOK:]], axis=1)
        before = jnp.logical_and(ti >= BLOCK, si < BLOCK)
        chosen = jnp.where(causal, scores[:, :TOK], jnp.where(before, cross, 0.0))
        within[span, :] = nn(chosen.astype(BF16), vbuf[span, :])
        cfull[span, :] = reader * jnp.exp(cfull[span, :])
    p2_relay(2)
    chunk = min(HEAD, (nz * ny * wo_cols))
    total_cols = chunk * nx
    src = lax.broadcasted_iota(jnp.int32, (total_cols, total_cols), 0)
    dst = lax.broadcasted_iota(jnp.int32, (total_cols, total_cols), 1)
    wanted = (
        lax.div(lax.rem(dst, 32), wo_cols) * chunk
        + lax.div(dst, 32) * wo_cols
        + lax.rem(dst, wo_cols)
    )
    order[...] = (src == wanted).astype(BF16)
    taken(c3_rs, c3_send.at[0 : ny - 1])
    gain = hg_ref[pl.ds(x, 1), :]

    def finish(s):
        span = slice(s * TOK, (s + 1) * TOK)
        prior = c3_recv[:, s * piece : (s + 1) * piece, :].reshape(HEAD, HEAD)
        read = within[span, :] + nt(cfull[span, :].astype(BF16), prior)
        square = jnp.mean(read * read, axis=-1, keepdims=True)
        normal = (read * lax.rsqrt(square + EPS) * gain).astype(BF16)
        xrec[x, s] = normal.reshape(2, HALF, HEAD)

    for s in range(nx):
        finish(s)
    to_all_x(lambda owner: xrec.at[owner], xr_ss, xr_rs)
    taken(xp_rs, xpool.at[0 : nx - 1])
    pieces = []
    for g in range(half_pool // WCOLS):
        cols = slice(g * WCOLS, (g + 1) * WCOLS)
        diff = jnp.concatenate(
            [xpool[2 * g + n].reshape(rows, HEAD) for n in range(2)], axis=1
        )
        pieces.append((nn(diff, maps_ref[g]) * scale_ref[:, cols]).astype(BF16))
    p2_wait(2)
    for p in range(2):
        both = wbuf[1, :, :, p].reshape(nz * ny, 2 * wo_cols, WCOLS).astype(F32)
        cols = slice(p * WCOLS, (p + 1) * WCOLS)
        wop[:, cols] = both[:, :wo_cols].reshape(nz * ny * wo_cols, WCOLS).astype(BF16)
        wor[:, cols] = both[:, wo_cols:].reshape(nz * ny * wo_cols, WCOLS).astype(BF16)
    pooled_out = nt(jnp.concatenate(pieces, axis=1), wop[...])
    pacc[...] = pooled_out.reshape(nx, 2, HALF, nz * ny * wo_cols)
    taken(xr_rs, xrec.at[0 : nx - 1])
    cols_out = nz * ny * wo_cols

    def to_half(s):
        return rc(parts.at[s, 1 - c], part_in.at[s], part_ss, part_rs.at[s], c=1 - c)

    def deliver(k, owner):
        to = at(x, k, nx)
        return rc(mixed.at[to], obuf.at[owner], o_ss, o_rs.at[k - 1], x=to)

    order_x = (*far_first(nx), 0)
    def half_of(core):
        rec = jnp.concatenate([xrec[i, :, core].reshape(nx * HALF, HEAD) for i in range(nx)], axis=1)
        pooled = pacc[:, core].reshape(nx * HALF, cols_out)
        parts[:, core] = (pooled + nt(rec, wor[...])).astype(BF16).reshape(nx, HALF, cols_out)

    half_of(1 - c)
    for k in order_x:
        to_half(at(x, k, nx)).start()
    half_of(c)
    for k in order_x:
        s = at(x, k, nx)
        to_half(s).wait_recv()
        joint = (parts[s, c].astype(F32) + part_in[s].astype(F32)).astype(BF16)
        if k:
            mixed[s] = joint
            deliver(k, x).start()
        else:
            obuf[x] = joint
    def reordered(owner):
        stacked = jnp.concatenate(
            [obuf[owner, :, q * chunk : (q + 1) * chunk] for q in range(cols_out // chunk)], axis=0
        )
        return nn(stacked, order[pl.ds(pl.multiple_of(owner * chunk, chunk), chunk), :])

    ordered = reordered(x)
    for k in (1, 3, 2):
        deliver(k, at(x, -k, nx)).wait_recv()
        ordered = ordered + reordered(at(x, -k, nx))
    ordered = ordered.astype(BF16)
    for q in range(cols_out // chunk):
        out_ref[0, :, q * total_cols : (q + 1) * total_cols] = ordered[q * HALF : (q + 1) * HALF]

    for st in range(3):
        p1_done(st)
        p2_done(st)
    left_here(tok_ss, tokbuf.at[0:3, 0])
    left_here(d2d_ss, tokbuf.at[:, 0])
    left_here(sp_ss, spbuf.at[0 : nx - 1])
    left_here(c1_ss, c1_send.at[0 : ny - 1])
    left_here(c3_ss, c3_send.at[0 : ny - 1])
    left_here(xp_ss, xpool.at[0 : nx - 1])
    left_here(xr_ss, xrec.at[0 : nx - 1])
    left_here(o_ss, mixed.at[0 : nx - 1])
    left_here(part_ss, part_in)
    if nz > 1:

        def sent_later(k, _):
            c2(k, z, z + k).wait_send()
            return _

        lax.fori_loop(1, nz - z, sent_later, 0)
    @pl.when(sp < last)
    def _():
        halo_copy(c=1 - c).wait_send()


def body(sizes, *arrays):
    nz, ny, nx = sizes
    (tok, gin, wp, wq, wf, wv, maps, scale, lb, spike, hg, wpo, wro) = arrays
    width = tok.shape[2]
    rows = nx * TOK
    piece = HEAD // ny
    packed = nx * piece
    wo_cols = 32 // nx
    cols_out = nz * ny * wo_cols
    kdim = nx * HEAD
    ring_inputs = [
        pltpu.VMEM(tok.shape, BF16),
        pltpu.VMEM((1, width), F32),
        pltpu.VMEM(maps.shape, BF16),
        pltpu.VMEM((1, kdim), F32),
        pltpu.VMEM((nx, HEAD), F32),
        pltpu.VMEM((1, spike.shape[2], TOK), F32),
        pltpu.VMEM((nx, HEAD), F32),
        pltpu.VMEM((2, 32, kdim), BF16),
    ]
    scratch = [
        *ring_inputs,
        pltpu.VMEM((nx, 2, HALF, width), BF16),
        pltpu.VMEM((2, nz, ny, 2, WROWS, WCOLS), BF16),
        pltpu.VMEM((2, nz, ny, 2 * WROWS, HEAD), BF16),
        pltpu.VMEM((2, 32, kdim), F32),
        pltpu.VMEM((cols_out, kdim), BF16),
        pltpu.VMEM((cols_out, kdim), BF16),
        pltpu.VMEM((nx, spike.shape[2], TOK), F32),
        pltpu.VMEM((rows, HEAD), BF16),
        pltpu.VMEM((rows, HEAD), BF16),
        pltpu.VMEM((rows, HEAD), BF16),
        pltpu.VMEM((nx, TOK, HEAD), BF16),
        pltpu.VMEM((rows, HEAD), F32),
        pltpu.VMEM((rows, HEAD), F32),
        pltpu.VMEM((ny, packed + 16, HEAD), BF16),
        pltpu.VMEM((ny, packed + 16, HEAD), BF16),
        pltpu.VMEM((ny, packed, HEAD), F32),
        pltpu.VMEM((ny, 8, HEAD), F32),
        pltpu.VMEM((packed + 16, HEAD), BF16),
        pltpu.VMEM((nz, packed + 16, HEAD), BF16),
        pltpu.VMEM((ny, packed, HEAD), BF16),
        pltpu.VMEM((ny, packed, HEAD), BF16),
        pltpu.VMEM((nx, HALO, HEAD), BF16),
        pltpu.VMEM((rows, HEAD), F32),
        pltpu.VMEM((nx, nx, TOK, HEAD), BF16),
        pltpu.VMEM((nx, nx, 2, HALF, HEAD), BF16),
        pltpu.VMEM((nx, 2, HALF, cols_out), F32),
        pltpu.VMEM((nx, 2, HALF, cols_out), BF16),
        pltpu.VMEM((nx, HALF, cols_out), BF16),
        pltpu.VMEM((nx, HALF, cols_out), BF16),
        pltpu.VMEM((nx, HALF, cols_out), BF16),
        pltpu.VMEM((nx * min(HEAD, cols_out), nx * min(HEAD, cols_out)), BF16),
        *[pltpu.SemaphoreType.DMA((3,))] * 2,
        pltpu.SemaphoreType.DMA((3,)),
        pltpu.SemaphoreType.DMA((3, PARTS)),
        pltpu.SemaphoreType.DMA((3, 2)),
        pltpu.SemaphoreType.DMA,
        pltpu.SemaphoreType.DMA((4,)),
        *[pltpu.SemaphoreType.DMA] * 2,
        *[pltpu.SemaphoreType.DMA] * 2,
        *[pltpu.SemaphoreType.DMA] * 2,
        *[pltpu.SemaphoreType.DMA((max(nz - 1, 1),))] * 2,
        *[pltpu.SemaphoreType.DMA] * 2,
        *[pltpu.SemaphoreType.DMA] * 2,
        *[pltpu.SemaphoreType.DMA] * 2,
        *[pltpu.SemaphoreType.DMA] * 2,
        pltpu.SemaphoreType.DMA,
        pltpu.SemaphoreType.DMA((nx,)),
        pltpu.SemaphoreType.DMA,
        pltpu.SemaphoreType.DMA((nx - 1,)),
        pltpu.SemaphoreType.DMA((10,)),
    ]
    return pl.pallas_call(
        functools.partial(kernel, sizes),
        out_shape=jax.ShapeDtypeStruct(tok.shape, BF16),
        in_specs=[pl.BlockSpec(memory_space=pltpu.HBM)] * 13,
        out_specs=pl.BlockSpec(memory_space=pltpu.VMEM),
        scratch_shapes=scratch,
        compiler_params=pltpu.CompilerParams(
            collective_id=0, has_side_effects=True, vmem_limit_bytes=40 * 1024 * 1024
        ),
        name="layer",
    )(*map(pinned, (
        tok,
        gin.reshape(1, width),
        wp,
        wq,
        wf,
        wv,
        maps,
        scale.reshape(1, kdim),
        lb.reshape(nx, HEAD),
        jnp.swapaxes(spike, 1, 2),
        hg.reshape(nx, HEAD),
        wpo.T,
        wro.T,
    )))


def pinned(array):
    return pltpu.with_memory_space_constraint(array, pltpu.HBM)


def layout(devices, sizes):
    nz, ny, nx = sizes
    torus = Mesh(devices.reshape(nz, ny, nx, 2), ("z", "y", "x", "c"))
    sp = ("z", "y")
    return jax.shard_map(
        functools.partial(body, sizes),
        mesh=torus,
        in_specs=(
            P("x", ("z", "y", "c"), None),
            P(),
            P(sp, "c"),
            P(sp, "c"),
            P(sp, "c"),
            P(sp, "c"),
            P("c", None, None),
            P("c"),
            P("c"),
            P("x", sp, "c"),
            P("c"),
            P("c", sp),
            P("c", sp),
        ),
        out_specs=P("x", ("z", "y", "c"), None),
        check_vma=False,
    )


def solution(mesh):
    return layout(mesh.devices, (8, 8, mesh.shape["fs"]))
```
